256 devices in a mesh: sp: 16 (over y, x), tp: 16 (over z, core).
Axes of the slice: x: 4, y: 4, z: 8, core: 2. Of those that a mesh axis runs over, the one named last changes fastest.
Arguments:
- stream: bfloat16 [2048, 16384], P('tp', 'sp'), may hold values from -12 to 12
- norm_gain: float32 [2, 2048], P(None, 'tp'), may hold values from 0.1 to 1.9
- in_weight: bfloat16 [2, 2048, 1024], P(None, 'sp', 'tp'), may hold values from -0.125 to 0.125
- out_weight: bfloat16 [2, 1024, 2048], P(None, 'tp', 'sp'), may hold values from -0.1875 to 0.1875
- docs: int32 [16384], P('sp'), may hold values from 0 to 3, never falling along the last dimension, each value on 1 to 8192 neighbouring positions
Outputs:
- mixed_out: bfloat16 [2048, 16384], P('tp', 'sp')
The draws below stay inside these ranges and needn't reach their ends.
Inputs may be any that keep to these rules, and one draw needn't show every extreme that they name: `docs`: numbers never fall along the positions and start at 0; a document spans at most 8192 positions.
All inputs are finite; a program needn't handle non-finite values.
Results may differ from the reference program's by a relative error of at most 0.0095.
Values may be sent and summed in bfloat16 or wider, within the bound.
A program may use at most 64 MiB of HBM per device.

```python
import math
import jax
import jax.numpy as jnp
import numpy as np
from jax import lax

D = 2048
PW = 1024
GROUPS = 4
WIDEST = 16
LAYERS = 2
TOKENS = 16384
DOCS = 4
DOC_MOST = 8192


def draw_stream(key, part):
    base_key, scale_key = jax.random.split(key)
    band_rows = D // 16
    base_draw = jnp.clip(jax.random.normal(base_key, (D, TOKENS), jnp.float32), -4.0, 4.0)
    levels = jnp.exp(jax.random.uniform(scale_key, (16, 1, 1), jnp.float32, jnp.log(0.3), jnp.log(3.0)))
    shaped = base_draw.reshape(16, band_rows, TOKENS) * levels
    return shaped.reshape(D, TOKENS).astype(jnp.bfloat16)


def steps_of(rng, shape, shards, low, high):
    factor_of, own = 1.0, jax.random.fold_in(rng, 6)
    for dim, shards_of in shards:
        steps = jnp.exp(jax.random.uniform(jax.random.fold_in(own, dim), (shards_of,), jnp.float32, low / len(shards), high / len(shards)))
        factor_of = factor_of * jnp.repeat(steps, shape[dim] // shards_of).reshape([-1 if axis == dim else 1 for axis in range(len(shape))])
    return factor_of


def split_up(amount, total, bound, skew):
    loads = [(1 << 20) // math.isqrt(grade ** skew) + 1 for grade in range(2, amount + 1)]
    rest, counts = total - bound - (amount - 1), [1] * (amount - 1)
    while rest > 0:
        candidates = [i for i in range(amount - 1) if counts[i] < bound]
        pool, left = sum([loads[i] for i in candidates]), rest
        for i in candidates:
            more = min(bound - counts[i], max(1, left * loads[i] // pool), rest)
            counts[i] = counts[i] + more
            rest = rest - more
    return np.array([bound] + counts)


def ragged(stream_key, count, total, limit, lean):
    if count == 2:
        one = jax.random.randint(stream_key, (), max(1, total - limit), min(limit, total - 1) + 1)
        return jnp.stack([one, total - one])
    lengths = jnp.asarray(split_up(count, total, limit, lean), jnp.int32)
    twos = (count - 1) // 2
    giver, taker = lengths[1:1 + 2 * twos:2], lengths[2:2 + 2 * twos:2]
    slack = jnp.minimum(giver - 1, limit - taker)
    moved = jax.random.randint(jax.random.fold_in(stream_key, 1), (twos,), 0, 1 << 20) % (slack + 1)
    lengths = lengths.at[1:1 + 2 * twos:2].set(giver - moved).at[2:2 + 2 * twos:2].set(taker + moved)
    return lengths[jax.random.permutation(jax.random.fold_in(stream_key, 2), count)]


def noise(stream_key, shape, scale, limit, cuts=(), kind=jnp.bfloat16):
    drawn = jax.random.normal(stream_key, shape, jnp.float32) * scale
    if len(cuts) > 0:
        drawn = steps_of(stream_key, shape, cuts, -0.22, 0.18) * drawn
    return jnp.clip(drawn, min=-limit, max=limit).astype(kind)


def setup_inputs(seed: int = 0) -> dict:
    streams_of = jax.random.split(jax.random.key(seed), 6)
    return {
        "stream": draw_stream(jax.random.fold_in(streams_of[5], 71), 0),
        "norm_gain": jnp.clip(1.0 + 0.18 * jax.random.normal(streams_of[1], (LAYERS, D), jnp.float32), 0.1, 1.9),
        "in_weight": noise(streams_of[2], (LAYERS, D, PW), D ** -0.5, 0.125, ((1, 16), (2, 16))),
        "out_weight": noise(streams_of[3], (LAYERS, PW, D), PW ** -0.5, 0.1875, ((1, 16), (2, 16))),
        "docs": jnp.searchsorted(jnp.cumsum(ragged(streams_of[4], DOCS, TOKENS, DOC_MOST, 1)), jnp.arange(TOKENS), side="right").astype(jnp.int32),
    }


def trailing_pool(values, docs, widths):
    length = values.shape[1]
    reach_back = WIDEST - 1
    extended = jnp.pad(values.astype(jnp.float32), ((0, 0), (reach_back, 0)))
    ext_docs = jnp.pad(docs + 1, (reach_back, 0))
    marker = docs + 1
    window_sum = jnp.zeros(values.shape, jnp.float32)
    members = jnp.zeros(values.shape, jnp.float32)
    for lag_step in range(WIDEST):
        lower_edge = reach_back - lag_step
        shifted = extended[:, lower_edge:lower_edge + length]
        same_doc = ext_docs[lower_edge:lower_edge + length] == marker
        inside = jnp.logical_and(same_doc[None, :], lag_step < widths[:, None])
        window_sum = window_sum + jnp.where(inside, shifted, jnp.float32(0.0))
        members = members + inside.astype(jnp.float32)
    return window_sum / members - values.astype(jnp.float32)

def reference(stream, norm_gain, in_weight, out_weight, docs):
    channel = lax.iota(jnp.int32, PW)
    widths = jnp.left_shift(jnp.int32(2), channel // (PW // GROUPS))
    residual = stream.astype(jnp.float32)
    for layer_idx in range(LAYERS):
        mean_square = lax.optimization_barrier(jnp.mean(residual * residual, axis=0))
        scaled = residual * lax.rsqrt(mean_square + 1e-06)[None, :] * norm_gain[layer_idx].astype(jnp.float32)[:, None]
        normed = scaled.astype(jnp.bfloat16)
        pool_in = jnp.dot(in_weight[layer_idx].T, normed, preferred_element_type=jnp.float32).astype(jnp.bfloat16)
        pooled = trailing_pool(pool_in, docs, widths).astype(jnp.bfloat16)
        residual = residual + jnp.dot(out_weight[layer_idx].T, pooled, preferred_element_type=jnp.float32)
    return residual.astype(jnp.bfloat16)
```

```python
import jax
import jax.numpy as jnp
from jax import lax
from jax.experimental import pallas as pl
from jax.experimental.pallas import tpu as pltpu
from jax.sharding import PartitionSpec as P

D = 2048
PW = 1024
LAYERS = 2
NY, NX, NZ = 4, 4, 8
TOK = 128
HALO = 32
ROWS = TOK + HALO
LANES = 128
WAVES = 4
HALF = 32

MESH = pl.DeviceIdType.MESH
NT = (((1,), (1,)), ((), ()))
NN = (((1,), (0,)), ((), ()))

STEP_OFFSETS = ((0,), (-1, 1), (-2, 2), (-3, 3), (4,))


def kernel(
    stream,
    gain,
    in_w,
    out_w,
    docs,
    out,
    weights,
    turned,
    taken,
    gains,
    own_gain,
    edge_docs,
    residual,
    sums_out,
    sums_in,
    last_out,
    last_in,
    mixed,
    masks,
    counts,
    plane_send,
    plane_recv,
    z_send,
    z_recv,
    line_send,
    line_recv,
    far_recv,
    take_send,
    take_recv,
    gain_send,
    gain_recv,
    edge_send,
    edge_recv,
    pair_send,
    pair_recv,
    sums_send,
    sums_recv,
    last_send,
    last_recv,
    mixed_send,
    mixed_recv,
):
    sp = lax.axis_index("sp")
    tp = lax.axis_index("tp")
    y, x = sp // NX, sp % NX
    z, core = tp // 2, tp % 2

    def at(yy, xx, zz):
        return (yy * NX + xx, zz * 2 + core)

    def turn(value, by, size):
        return (value + by + size) % size

    sibling = (sp, z * 2 + 1 - core)
    has_next = jnp.logical_and(z == NZ - 1, sp < NY * NX - 1)
    has_edge = jnp.logical_and(z == 0, sp > 0)

    def copy(src, dst, send, recv, device):
        return pltpu.make_async_remote_copy(
            src_ref=src, dst_ref=dst, send_sem=send, recv_sem=recv, device_id=device, device_id_type=MESH
        )

    def drain(ref, sem):
        pltpu.make_async_copy(ref, ref, sem).wait()

    barrier = pltpu.get_barrier_semaphore()
    peers = [at(turn(y, d, NY), x, z) for d in range(1, NY)]
    peers += [at(y, turn(x, d, NX), z) for d in range(1, NX)]
    peers += [at(y, x, turn(z, d, NZ)) for d in range(1, NZ)]
    peers += [sibling]
    for peer in peers:
        pl.semaphore_signal(barrier, inc=1, device_id=peer, device_id_type=MESH)

    @pl.when(has_next)
    def _():
        pl.semaphore_signal(barrier, inc=1, device_id=(sp + 1, core), device_id_type=MESH)

    @pl.when(has_edge)
    def _():
        pl.semaphore_signal(
            barrier, inc=1, device_id=(sp - 1, (NZ - 1) * 2 + core), device_id_type=MESH
        )

    for layer in range(LAYERS):
        weights[2 * layer, y, x, z] = in_w[layer].astype(jnp.float32).T.astype(jnp.bfloat16)
        weights[2 * layer + 1, y, x, z] = out_w[layer]
    for j in range(NZ):
        block = stream[:, j * TOK : (j + 1) * TOK].astype(jnp.float32)
        turned[j * TOK : (j + 1) * TOK, :] = block.T.astype(jnp.bfloat16)
    own_gain[...] = jnp.zeros_like(own_gain)
    own_gain[0:LAYERS, :] = gain[...]

    extra = jnp.logical_or(has_next, has_edge).astype(jnp.int32)
    pl.semaphore_wait(barrier, len(peers) + extra)

    for d in range(1, NY):
        part = weights.at[:, y, x, z, 0:HALF, :]
        copy(part, part, plane_send, plane_recv, at(turn(y, d, NY), x, z)).start()
    for d in range(1, NX):
        part = weights.at[:, y, x, z, HALF : 2 * HALF, :]
        copy(part, part, plane_send, plane_recv, at(y, turn(x, d, NX), z)).start()

    def slab_a(w, xx, zz):
        return weights.at[w, :, xx, zz, 0:HALF, :]

    def slab_b(w, yy, zz):
        return weights.at[w, yy, :, zz, HALF : 2 * HALF, :]

    def send_z(w, step):
        up, down = at(y, x, turn(z, 1, NZ)), at(y, x, turn(z, -1, NZ))
        before, after = turn(z, -step, NZ), turn(z, step, NZ)
        send, recv = z_send.at[w], z_recv.at[w, step]
        a, b = slab_a(w, x, before), slab_b(w, y, after)
        copy(a, a, send, recv, up).start()
        copy(b, b, send, recv, down).start()
        if step < 3:
            a, b = slab_a(w, x, after), slab_b(w, y, before)
            copy(a, a, send, recv, down).start()
            copy(b, b, send, recv, up).start()

    def wait_z(w, step):
        drain(weights.at[w, 0, 0, 0 : (8 if step < 4 else 4)], z_recv.at[w, step - 1])

    def send_line(w, step):
        for offset in STEP_OFFSETS[step]:
            zz = turn(z, offset, NZ)
            a, b = slab_a(w, x, zz), slab_b(w, y, zz)
            for side in (1, -1):
                copy(a, a, line_send.at[w], line_recv.at[w, step], at(y, turn(x, side, NX), z)).start()
                copy(b, b, line_send.at[w], line_recv.at[w, step], at(turn(y, side, NY), x, z)).start()

    def pass_on(w, step):
        drain(weights.at[w, 0, 0 : len(STEP_OFFSETS[step])], line_recv.at[w, step])
        for offset in STEP_OFFSETS[step]:
            zz = turn(z, offset, NZ)
            ahead = 1 - 2 * (zz % 2)
            a, b = slab_a(w, turn(x, -ahead, NX), zz), slab_b(w, turn(y, -ahead, NY), zz)
            copy(a, a, line_send.at[w], far_recv.at[w], at(y, turn(x, ahead, NX), z)).start()
            copy(b, b, line_send.at[w], far_recv.at[w], at(turn(y, ahead, NY), x, z)).start()

    def wait_far(w):
        drain(weights.at[w, 0], far_recv.at[w])

    def send_taken(d):
        zz = turn(z, d, NZ)
        target = at(y, x, zz)
        copy(own_gain, gains.at[core, z], gain_send, gain_recv, target).start()

        @pl.when(zz == 0)
        def _():
            copy(
                turned.at[0:TOK, :], taken.at[core, z, HALO:ROWS, :], take_send, take_recv, target
            ).start()

        @pl.when(zz > 0)
        def _():
            first = pl.multiple_of(jnp.maximum(zz * TOK - HALO, 0), 32)
            copy(
                turned.at[pl.ds(first, ROWS), :], taken.at[core, z], take_send, take_recv, target
            ).start()

    def gather_stream():
        gains[core, z] = own_gain[...]

        @pl.when(z == 0)
        def _():
            taken[core, z, HALO:ROWS, :] = turned[0:TOK, :]

        @pl.when(z > 0)
        def _():
            first = pl.multiple_of(jnp.maximum(z * TOK - HALO, 0), 32)
            taken[core, z] = turned[pl.ds(first, ROWS), :]

        drain(gains.at[0, 0:7], gain_recv)

        @pl.when(z == 0)
        def _():
            drain(taken.at[0, 0:7, HALO:ROWS, :], take_recv)

        @pl.when(z > 0)
        def _():
            drain(taken.at[0, 0:7], take_recv)

        to_next = copy(
            taken.at[core, :, TOK:ROWS, :],
            taken.at[core, :, 0:HALO, :],
            edge_send.at[0],
            edge_recv.at[0],
            (sp + 1, core),
        )
        docs_next = copy(docs, edge_docs, edge_send.at[1], edge_recv.at[1], (sp + 1, core))

        @pl.when(has_next)
        def _():
            to_next.start()
            docs_next.start()
            to_next.wait_send()
            docs_next.wait_send()

        @pl.when(has_edge)
        def _():
            to_next.wait_recv()
            docs_next.wait_recv()

        @pl.when(jnp.logical_and(z == 0, sp == 0))
        def _():
            taken[core, :, 0:HALO, :] = jnp.zeros((NZ, HALO, LANES), jnp.bfloat16)
            edge_docs[...] = jnp.full(edge_docs.shape, -1, jnp.int32)

        mine = taken.at[core]
        copy(mine, mine, pair_send.at[0], pair_recv.at[0], sibling).start()
        mine = gains.at[core]
        copy(mine, mine, pair_send.at[1], pair_recv.at[1], sibling).start()

    def windows():
        own = docs[pl.ds(z, 1), :].astype(jnp.float32)
        inside = docs[pl.ds(turn(z, -1, NZ), 1), :].astype(jnp.float32)

        def stood(row):
            return jnp.broadcast_to(row, (LANES, LANES)).T

        masks[HALO:ROWS, :] = stood(own)

        @pl.when(z > 0)
        def _():
            masks[0:HALO, :] = stood(inside)[LANES - HALO :, :]

        @pl.when(z == 0)
        def _():
            masks[0:HALO, :] = stood(edge_docs[NZ - 1 : NZ, :].astype(jnp.float32))[LANES - HALO :, :]

        column = masks[...]
        members = jnp.ones((ROWS, LANES), jnp.float32)
        for g in range(4):
            same = column == pltpu.roll(column, 2**g, 0)
            members = members + jnp.where(same, pltpu.roll(members, 2**g, 0), 0.0)
            counts[g] = members

    def same_doc(g):
        column = masks[...]
        return column == pltpu.roll(column, 2**g, 0)

    def block_of(k):
        return k % 2, k // 2

    def stream_in():
        pltpu.make_async_copy(taken.at[0], taken.at[0], pair_recv.at[0]).wait()
        pltpu.make_async_copy(gains.at[0], gains.at[0], pair_recv.at[1]).wait()
        for k in range(16):
            residual[block_of(k)] = taken[block_of(k)].astype(jnp.float32)

    def pooled_of(layer):
        squares = jnp.zeros((ROWS, LANES), jnp.float32)
        for k in range(16):
            r = residual[block_of(k)]
            squares = squares + r * r
        mean = jnp.sum(squares, axis=1, keepdims=True) * (1.0 / D)
        scale = lax.rsqrt(mean + 1e-06)
        total = jnp.zeros((ROWS, PW // 2), jnp.float32)
        for j in range(8):
            pieces, sides = [], []
            for k in (2 * j, 2 * j + 1):
                g = gains[k % 2, k // 2, layer : layer + 1, :]
                pieces.append((residual[block_of(k)] * scale * g).astype(jnp.bfloat16))
                sides.append(weights[2 * layer, k // NX, k % NX].reshape(PW // 2, LANES))
            total = total + lax.dot_general(
                jnp.concatenate(pieces, axis=1),
                jnp.concatenate(sides, axis=1),
                NT,
                preferred_element_type=jnp.float32,
            )
        pool_in = total.astype(jnp.bfloat16).astype(jnp.float32)
        groups = []
        for g in range(4):
            values = pool_in[:, g * LANES : (g + 1) * LANES]
            window = values
            for h in range(g + 1):
                window = window + jnp.where(same_doc(h), pltpu.roll(window, 2**h, 0), 0.0)
            groups.append((window / counts[g] - values).astype(jnp.bfloat16))
        return jnp.concatenate(groups, axis=1)

    def project_out(pooled):
        for j in range(8):
            side = [weights[1, k // NX, k % NX].reshape(PW // 2, LANES) for k in (2 * j, 2 * j + 1)]
            part = lax.dot_general(
                pooled, jnp.concatenate(side, axis=1), NN, preferred_element_type=jnp.float32
            )
            for h in range(2):
                piece = part[:, h * LANES : (h + 1) * LANES]
                residual[h, j] = residual[h, j] + piece
                sums_out[j, h] = piece.astype(jnp.bfloat16)
            if j % 2 == 1:
                pair = pl.ds(j - 1, 2)
                copy(
                    sums_out.at[pair], sums_in.at[pair], sums_send.at[j // 2], sums_recv.at[j // 2], sibling
                ).start()

    def add_sums():
        for q in range(4):
            pair = pl.ds(2 * q, 2)
            pltpu.make_async_copy(sums_in.at[pair], sums_in.at[pair], sums_recv.at[q]).wait()
            for j in (2 * q, 2 * q + 1):
                for h in range(2):
                    residual[h, j] = residual[h, j] + sums_in[j, h].astype(jnp.float32)

    order = (4, 3, 5, 2, 6, 1, 7, 0)

    def project_last(pooled):
        tail = pooled[HALO:, :]
        for i, d in enumerate(order):
            j = turn(z, d, NZ)
            yy, xx = j // 2, 2 * (j % 2)
            side = [weights[3, yy, xx + h].reshape(PW // 2, LANES) for h in range(2)]
            part = lax.dot_general(
                tail, jnp.concatenate(side, axis=1), NN, preferred_element_type=jnp.float32
            )
            low, high = part[:, :LANES], part[:, LANES:]
            last_out[i] = jnp.where(core == 0, high, low).astype(jnp.bfloat16)
            copy(last_out.at[i], last_in.at[i], last_send.at[i], last_recv.at[i], sibling).start()
            residual[core, j, HALO:ROWS, :] = residual[core, j, HALO:ROWS, :] + jnp.where(core == 0, low, high)
        lanes = pl.ds(pl.multiple_of(z * TOK, TOK), TOK)
        for i, d in enumerate(order):
            j = turn(z, d, NZ)
            pltpu.make_async_copy(last_in.at[i], last_in.at[i], last_recv.at[i]).wait()
            done = residual[core, j, HALO:ROWS, :] + last_in[i].astype(jnp.float32)
            if d == 0:
                out[:, lanes] = done.T.astype(jnp.bfloat16)
            else:
                mixed[i] = done.T.astype(jnp.bfloat16)
                copy(mixed.at[i], out.at[:, lanes], mixed_send, mixed_recv, at(y, x, j)).start()

    drain(weights.at[0, 0, 0:2, 0:6], plane_recv)
    send_z(0, 0)
    send_line(0, 0)
    pooled = None
    for w in range(WAVES):
        for step in range(1, 5):
            wait_z(w, step)
            if step < 4:
                send_z(w, step)
            if step == 2 and w + 1 < WAVES:
                send_z(w + 1, 0)
            send_line(w, step)
            pass_on(w, step - 1)
            if w == 0:
                for d in ((1, 7), (2, 6), (3, 5), (4,))[step - 1]:
                    send_taken(d)
            if w == 1 and step == 1:
                gather_stream()
                windows()
            if w > 0 and step == 2:
                wait_far(w - 1)
                if w == 1:
                    stream_in()
                    pooled = pooled_of(0)
                if w == 2:
                    project_out(pooled)
                if w == 3:
                    add_sums()
                    pooled = pooled_of(1)
            if step == 4 and w + 1 < WAVES:
                send_line(w + 1, 0)
        pass_on(w, 4)
    wait_far(3)
    project_last(pooled)

    drain(out.at[:, 0 : 7 * TOK], mixed_recv)
    drain(mixed.at[0:7], mixed_send)
    drain(weights.at[0, 0, 0:2, 0:6], plane_send)
    for w in range(WAVES):
        drain(weights.at[w, 0, :, 0:7], z_send.at[w])
        drain(weights.at[w, 0:3], line_send.at[w])
    drain(gains.at[0, 0:7], gain_send)

    @pl.when(z == 0)
    def _():
        drain(taken.at[0, 0:7], take_send)

    @pl.when(z > 0)
    def _():
        drain(taken.at[0, :, 0 : ROWS - 24, :], take_send)

    pltpu.make_async_copy(taken.at[0], taken.at[0], pair_send.at[0]).wait()
    pltpu.make_async_copy(gains.at[0], gains.at[0], pair_send.at[1]).wait()
    for q in range(4):
        pair = pl.ds(2 * q, 2)
        pltpu.make_async_copy(sums_out.at[pair], sums_out.at[pair], sums_send.at[q]).wait()
    for i in range(8):
        pltpu.make_async_copy(last_out.at[i], last_out.at[i], last_send.at[i]).wait()


def per_device(stream, norm_gain, in_weight, out_weight, docs):
    vmem = pl.BlockSpec(memory_space=pltpu.VMEM)
    dma = pltpu.SemaphoreType.DMA
    bf16, f32 = jnp.bfloat16, jnp.float32
    return pl.pallas_call(
        kernel,
        out_shape=jax.ShapeDtypeStruct(stream.shape, bf16),
        in_specs=[vmem] * 5,
        out_specs=vmem,
        scratch_shapes=[
            pltpu.VMEM((WAVES, NY, NX, NZ, 64, LANES), bf16),
            pltpu.VMEM((NZ * TOK, LANES), bf16),
            pltpu.VMEM((2, NZ, ROWS, LANES), bf16),
            pltpu.VMEM((2, NZ, 8, LANES), f32),
            pltpu.VMEM((8, LANES), f32),
            pltpu.VMEM((NZ, LANES), jnp.int32),
            pltpu.VMEM((2, NZ, ROWS, LANES), f32),
            pltpu.VMEM((NZ, 2, ROWS, LANES), bf16),
            pltpu.VMEM((NZ, 2, ROWS, LANES), bf16),
            pltpu.VMEM((NZ, TOK, LANES), bf16),
            pltpu.VMEM((NZ, TOK, LANES), bf16),
            pltpu.VMEM((NZ, TOK, LANES), bf16),
            pltpu.VMEM((ROWS, LANES), f32),
            pltpu.VMEM((4, ROWS, LANES), f32),
            dma,
            dma,
            dma((WAVES,)),
            dma((WAVES, 4)),
            dma((WAVES,)),
            dma((WAVES, 5)),
            dma((WAVES,)),
            dma,
            dma,
            dma,
            dma,
            dma((2,)),
            dma((2,)),
            dma((2,)),
            dma((2,)),
            dma((4,)),
            dma((4,)),
            dma((8,)),
            dma((8,)),
            dma,
            dma,
        ],
        compiler_params=pltpu.CompilerParams(collective_id=0, has_side_effects=True),
    )(stream, norm_gain, in_weight, out_weight, docs.reshape(NZ, LANES))


def solution(mesh):
    return jax.shard_map(
        per_device,
        mesh=mesh,
        in_specs=(P("tp", "sp"), P(None, "tp"), P(None, "sp", "tp"), P(None, "tp", "sp"), P("sp")),
        out_specs=P("tp", "sp"),
        check_vma=False,
    )
```

```python
import jax
import jax.numpy as jnp
from jax import lax
from jax.experimental import pallas as pl
from jax.experimental.pallas import tpu as pltpu
from jax.sharding import PartitionSpec as P

D = 2048
PW = 1024
LAYERS = 2
NY, NX, NZ = 4, 4, 8
TOK = 128
HALO = 32
ROWS = TOK + HALO
LANES = 128
WAVES = 4
HALF = 32

MESH = pl.DeviceIdType.MESH
NT = (((1,), (1,)), ((), ()))
NN = (((1,), (0,)), ((), ()))

STEP_OFFSETS = ((0,), (-1, 1), (-2, 2), (-3, 3), (4,))


def kernel(
    stream,
    gain,
    in_w,
    out_w,
    docs,
    out,
    weights,
    turned,
    taken,
    gains,
    own_gain,
    edge_docs,
    residual,
    sums_out,
    sums_in,
    last_out,
    last_in,
    mixed,
    masks,
    counts,
    plane_send,
    plane_recv,
    z_send,
    z_recv,
    line_send,
    line_recv,
    far_recv,
    take_send,
    take_recv,
    gain_send,
    gain_recv,
    edge_send,
    edge_recv,
    pair_send,
    pair_recv,
    sums_send,
    sums_recv,
    last_send,
    last_recv,
    mixed_send,
    mixed_recv,
):
    sp = lax.axis_index("sp")
    tp = lax.axis_index("tp")
    y, x = sp // NX, sp % NX
    z, core = tp // 2, tp % 2

    def at(yy, xx, zz):
        return (yy * NX + xx, zz * 2 + core)

    def turn(value, by, size):
        return (value + by + size) % size

    sibling = (sp, z * 2 + 1 - core)
    has_next = jnp.logical_and(z == NZ - 1, sp < NY * NX - 1)
    has_edge = jnp.logical_and(z == 0, sp > 0)

    def copy(src, dst, send, recv, device):
        return pltpu.make_async_remote_copy(
            src_ref=src, dst_ref=dst, send_sem=send, recv_sem=recv, device_id=device, device_id_type=MESH
        )

    def drain(ref, sem):
        pltpu.make_async_copy(ref, ref, sem).wait()

    barrier = pltpu.get_barrier_semaphore()
    peers = [at(turn(y, d, NY), x, z) for d in range(1, NY)]
    peers += [at(y, turn(x, d, NX), z) for d in range(1, NX)]
    peers += [at(y, x, turn(z, d, NZ)) for d in range(1, NZ)]
    peers += [sibling]
    for peer in peers:
        pl.semaphore_signal(barrier, inc=1, device_id=peer, device_id_type=MESH)

    @pl.when(has_next)
    def _():
        pl.semaphore_signal(barrier, inc=1, device_id=(sp + 1, core), device_id_type=MESH)

    @pl.when(has_edge)
    def _():
        pl.semaphore_signal(
            barrier, inc=1, device_id=(sp - 1, (NZ - 1) * 2 + core), device_id_type=MESH
        )

    for layer in range(LAYERS):
        weights[2 * layer, y, x, z] = in_w[layer]
        weights[2 * layer + 1, y, x, z] = out_w[layer]
    for j in range(NZ):
        block = stream[:, j * TOK : (j + 1) * TOK].astype(jnp.float32)
        turned[j * TOK : (j + 1) * TOK, :] = block.T.astype(jnp.bfloat16)
    own_gain[...] = jnp.zeros_like(own_gain)
    own_gain[0:LAYERS, :] = gain[...]

    extra = jnp.logical_or(has_next, has_edge).astype(jnp.int32)
    pl.semaphore_wait(barrier, len(peers) + extra)

    for group, waves in enumerate((slice(0, 1), slice(1, WAVES))):
        for d in range(1, NY):
            part = weights.at[waves, y, x, z, 0:HALF, :]
            copy(part, part, plane_send, plane_recv.at[group], at(turn(y, d, NY), x, z)).start()
        for d in range(1, NX):
            part = weights.at[waves, y, x, z, HALF : 2 * HALF, :]
            copy(part, part, plane_send, plane_recv.at[group], at(y, turn(x, d, NX), z)).start()

    def slab_a(w, xx, zz):
        return weights.at[w, :, xx, zz, 0:HALF, :]

    def slab_b(w, yy, zz):
        return weights.at[w, yy, :, zz, HALF : 2 * HALF, :]

    def send_z(w, step):
        up, down = at(y, x, turn(z, 1, NZ)), at(y, x, turn(z, -1, NZ))
        before, after = turn(z, -step, NZ), turn(z, step, NZ)
        send, recv = z_send.at[w], z_recv.at[w, step]
        a, b = slab_a(w, x, before), slab_b(w, y, after)
        copy(a, a, send, recv, up).start()
        copy(b, b, send, recv, down).start()
        if step < 3:
            a, b = slab_a(w, x, after), slab_b(w, y, before)
            copy(a, a, send, recv, down).start()
            copy(b, b, send, recv, up).start()

    def wait_z(w, step):
        drain(weights.at[w, 0, 0, 0 : (8 if step < 4 else 4)], z_recv.at[w, step - 1])

    def send_line(w, step):
        for offset in STEP_OFFSETS[step]:
            zz = turn(z, offset, NZ)
            a, b = slab_a(w, x, zz), slab_b(w, y, zz)
            for side in (1, -1):
                copy(a, a, line_send.at[w], line_recv.at[w, step], at(y, turn(x, side, NX), z)).start()
                copy(b, b, line_send.at[w], line_recv.at[w, step], at(turn(y, side, NY), x, z)).start()

    def pass_on(w, step):
        drain(weights.at[w, 0, 0 : len(STEP_OFFSETS[step])], line_recv.at[w, step])
        for offset in STEP_OFFSETS[step]:
            zz = turn(z, offset, NZ)
            ahead = 1 - 2 * (zz % 2)
            a, b = slab_a(w, turn(x, -ahead, NX), zz), slab_b(w, turn(y, -ahead, NY), zz)
            copy(a, a, line_send.at[w], far_recv.at[w], at(y, turn(x, ahead, NX), z)).start()
            copy(b, b, line_send.at[w], far_recv.at[w], at(turn(y, ahead, NY), x, z)).start()

    def wait_far(w):
        drain(weights.at[w, 0], far_recv.at[w])

    def send_taken(d):
        zz = turn(z, d, NZ)
        target = at(y, x, zz)
        copy(own_gain, gains.at[core, z], gain_send, gain_recv, target).start()

        @pl.when(zz == 0)
        def _():
            copy(
                turned.at[0:TOK, :], taken.at[core, z, HALO:ROWS, :], take_send, take_recv, target
            ).start()

        @pl.when(zz > 0)
        def _():
            first = pl.multiple_of(jnp.maximum(zz * TOK - HALO, 0), 32)
            copy(
                turned.at[pl.ds(first, ROWS), :], taken.at[core, z], take_send, take_recv, target
            ).start()

    def gather_stream():
        gains[core, z] = own_gain[...]

        @pl.when(z == 0)
        def _():
            taken[core, z, HALO:ROWS, :] = turned[0:TOK, :]

        @pl.when(z > 0)
        def _():
            first = pl.multiple_of(jnp.maximum(z * TOK - HALO, 0), 32)
            taken[core, z] = turned[pl.ds(first, ROWS), :]

        drain(gains.at[0, 0:7], gain_recv)

        @pl.when(z == 0)
        def _():
            drain(taken.at[0, 0:7, HALO:ROWS, :], take_recv)

        @pl.when(z > 0)
        def _():
            drain(taken.at[0, 0:7], take_recv)

        to_next = copy(
            taken.at[core, :, TOK:ROWS, :],
            taken.at[core, :, 0:HALO, :],
            edge_send.at[0],
            edge_recv.at[0],
            (sp + 1, core),
        )
        docs_next = copy(docs, edge_docs, edge_send.at[1], edge_recv.at[1], (sp + 1, core))

        @pl.when(has_next)
        def _():
            to_next.start()
            docs_next.start()
            to_next.wait_send()
            docs_next.wait_send()

        @pl.when(has_edge)
        def _():
            to_next.wait_recv()
            docs_next.wait_recv()

        @pl.when(jnp.logical_and(z == 0, sp == 0))
        def _():
            taken[core, :, 0:HALO, :] = jnp.zeros((NZ, HALO, LANES), jnp.bfloat16)
            edge_docs[...] = jnp.full(edge_docs.shape, -1, jnp.int32)

        mine = taken.at[core]
        copy(mine, mine, pair_send.at[0], pair_recv.at[0], sibling).start()
        mine = gains.at[core]
        copy(mine, mine, pair_send.at[1], pair_recv.at[1], sibling).start()

    def windows():
        own = docs[pl.ds(z, 1), :].astype(jnp.float32)
        inside = docs[pl.ds(turn(z, -1, NZ), 1), :].astype(jnp.float32)

        def stood(row):
            return jnp.broadcast_to(row, (LANES, LANES)).T

        masks[HALO:ROWS, :] = stood(own)

        @pl.when(z > 0)
        def _():
            masks[0:HALO, :] = stood(inside)[LANES - HALO :, :]

        @pl.when(z == 0)
        def _():
            masks[0:HALO, :] = stood(edge_docs[NZ - 1 : NZ, :].astype(jnp.float32))[LANES - HALO :, :]

        column = masks[...]
        members = jnp.ones((ROWS, LANES), jnp.float32)
        for g in range(4):
            same = column == pltpu.roll(column, 2**g, 0)
            members = members + jnp.where(same, pltpu.roll(members, 2**g, 0), 0.0)
            counts[g] = members

    def same_doc(g):
        column = masks[...]
        return column == pltpu.roll(column, 2**g, 0)

    def block_of(k):
        return k % 2, k // 2

    def stream_in():
        pltpu.make_async_copy(taken.at[0], taken.at[0], pair_recv.at[0]).wait()
        pltpu.make_async_copy(gains.at[0], gains.at[0], pair_recv.at[1]).wait()
        for k in range(16):
            residual[block_of(k)] = taken[block_of(k)].astype(jnp.float32)

    def pooled_of(layer):
        squares = jnp.zeros((ROWS, LANES), jnp.float32)
        for k in range(16):
            r = residual[block_of(k)]
            squares = squares + r * r
        mean = jnp.sum(squares, axis=1, keepdims=True) * (1.0 / D)
        scale = lax.rsqrt(mean + 1e-06)
        total = jnp.zeros((ROWS, PW // 2), jnp.float32)
        for j in range(8):
            pieces, sides = [], []
            for k in (2 * j, 2 * j + 1):
                g = gains[k % 2, k // 2, layer : layer + 1, :]
                pieces.append((residual[block_of(k)] * scale * g).astype(jnp.bfloat16))
                sides.append(weights[2 * layer, k // NX, k % NX].reshape(PW // 2, LANES))
            total = total + lax.dot_general(
                jnp.concatenate(pieces, axis=1),
                jnp.concatenate(sides, axis=1),
                NT,
                preferred_element_type=jnp.float32,
            )
        pool_in = total.astype(jnp.bfloat16).astype(jnp.float32)
        groups = []
        for g in range(4):
            values = pool_in[:, g * LANES : (g + 1) * LANES]
            window = values
            for h in range(g + 1):
                window = window + jnp.where(same_doc(h), pltpu.roll(window, 2**h, 0), 0.0)
            groups.append((window / counts[g] - values).astype(jnp.bfloat16))
        return jnp.concatenate(groups, axis=1)

    def project_out(pooled):
        for j in range(8):
            side = [weights[1, k // NX, k % NX].reshape(PW // 2, LANES) for k in (2 * j, 2 * j + 1)]
            part = lax.dot_general(
                pooled, jnp.concatenate(side, axis=1), NN, preferred_element_type=jnp.float32
            )
            for h in range(2):
                piece = part[:, h * LANES : (h + 1) * LANES]
                residual[h, j] = residual[h, j] + piece
                sums_out[j, h] = piece.astype(jnp.bfloat16)
            if j % 2 == 1:
                pair = pl.ds(j - 1, 2)
                copy(
                    sums_out.at[pair], sums_in.at[pair], sums_send.at[j // 2], sums_recv.at[j // 2], sibling
                ).start()

    def add_sums():
        for q in range(4):
            pair = pl.ds(2 * q, 2)
            pltpu.make_async_copy(sums_in.at[pair], sums_in.at[pair], sums_recv.at[q]).wait()
            for j in (2 * q, 2 * q + 1):
                for h in range(2):
                    residual[h, j] = residual[h, j] + sums_in[j, h].astype(jnp.float32)

    order = (4, 3, 5, 2, 6, 1, 7, 0)

    def project_last(pooled):
        tail = pooled[HALO:, :]
        for i, d in enumerate(order):
            j = turn(z, d, NZ)
            yy, xx = j // 2, 2 * (j % 2)
            side = [weights[3, yy, xx + h].reshape(PW // 2, LANES) for h in range(2)]
            part = lax.dot_general(
                tail, jnp.concatenate(side, axis=1), NN, preferred_element_type=jnp.float32
            )
            low, high = part[:, :LANES], part[:, LANES:]
            last_out[i] = jnp.where(core == 0, high, low).astype(jnp.bfloat16)
            copy(last_out.at[i], last_in.at[i], last_send.at[i], last_recv.at[i], sibling).start()
            residual[core, j, HALO:ROWS, :] = residual[core, j, HALO:ROWS, :] + jnp.where(core == 0, low, high)
        lanes = pl.ds(pl.multiple_of(z * TOK, TOK), TOK)
        for i, d in enumerate(order):
            j = turn(z, d, NZ)
            pltpu.make_async_copy(last_in.at[i], last_in.at[i], last_recv.at[i]).wait()
            done = residual[core, j, HALO:ROWS, :] + last_in[i].astype(jnp.float32)
            if d == 0:
                out[:, lanes] = done.T.astype(jnp.bfloat16)
            else:
                mixed[i] = done.T.astype(jnp.bfloat16)
                copy(mixed.at[i], out.at[:, lanes], mixed_send, mixed_recv, at(y, x, j)).start()

    drain(weights.at[0, 0, 0, 0:3], plane_recv.at[0])
    send_z(0, 0)
    send_line(0, 0)
    drain(weights.at[0, 0, 0:3, 0:3], plane_recv.at[1])
    send_z(1, 0)
    send_line(1, 0)

    def pass_on_tick(tick):
        for w in range(WAVES):
            if 0 <= tick - w <= 4:
                pass_on(w, tick - w)

    for tick in range(1, WAVES + 4):
        for w in range(WAVES):
            step = tick - w
            if 1 <= step <= 4:
                wait_z(w, step)
                if step < 4:
                    send_z(w, step)
                send_line(w, step)
        if tick + 1 < WAVES:
            send_z(tick + 1, 0)
            send_line(tick + 1, 0)
        if tick <= 4:
            for d in ((1, 7), (2, 6), (3, 5), (4,))[tick - 1]:
                send_taken(d)
        if tick >= 2:
            pass_on_tick(tick - 2)
        if tick == 6:
            gather_stream()
            windows()
    wait_far(0)
    stream_in()
    pooled = pooled_of(0)
    pass_on_tick(6)
    wait_far(1)
    project_out(pooled)
    pass_on_tick(7)
    wait_far(2)
    add_sums()
    pooled = pooled_of(1)
    wait_far(3)
    project_last(pooled)

    drain(out.at[:, 0 : 7 * TOK], mixed_recv)
    drain(mixed.at[0:7], mixed_send)
    drain(weights.at[0, 0, 0:2, 0:6], plane_send)
    for w in range(WAVES):
        drain(weights.at[w, 0, :, 0:7], z_send.at[w])
        drain(weights.at[w, 0:3], line_send.at[w])
    drain(gains.at[0, 0:7], gain_send)

    @pl.when(z == 0)
    def _():
        drain(taken.at[0, 0:7], take_send)

    @pl.when(z > 0)
    def _():
        drain(taken.at[0, :, 0 : ROWS - 24, :], take_send)

    pltpu.make_async_copy(taken.at[0], taken.at[0], pair_send.at[0]).wait()
    pltpu.make_async_copy(gains.at[0], gains.at[0], pair_send.at[1]).wait()
    for q in range(4):
        pair = pl.ds(2 * q, 2)
        pltpu.make_async_copy(sums_out.at[pair], sums_out.at[pair], sums_send.at[q]).wait()
    for i in range(8):
        pltpu.make_async_copy(last_out.at[i], last_out.at[i], last_send.at[i]).wait()


def per_device(stream, norm_gain, in_weight, out_weight, docs):
    vmem = pl.BlockSpec(memory_space=pltpu.VMEM)
    dma = pltpu.SemaphoreType.DMA
    bf16, f32 = jnp.bfloat16, jnp.float32
    return pl.pallas_call(
        kernel,
        out_shape=jax.ShapeDtypeStruct(stream.shape, bf16),
        in_specs=[vmem] * 5,
        out_specs=vmem,
        scratch_shapes=[
            pltpu.VMEM((WAVES, NY, NX, NZ, 64, LANES), bf16),
            pltpu.VMEM((NZ * TOK, LANES), bf16),
            pltpu.VMEM((2, NZ, ROWS, LANES), bf16),
            pltpu.VMEM((2, NZ, 8, LANES), f32),
            pltpu.VMEM((8, LANES), f32),
            pltpu.VMEM((NZ, LANES), jnp.int32),
            pltpu.VMEM((2, NZ, ROWS, LANES), f32),
            pltpu.VMEM((NZ, 2, ROWS, LANES), bf16),
            pltpu.VMEM((NZ, 2, ROWS, LANES), bf16),
            pltpu.VMEM((NZ, TOK, LANES), bf16),
            pltpu.VMEM((NZ, TOK, LANES), bf16),
            pltpu.VMEM((NZ, TOK, LANES), bf16),
            pltpu.VMEM((ROWS, LANES), f32),
            pltpu.VMEM((4, ROWS, LANES), f32),
            dma,
            dma((2,)),
            dma((WAVES,)),
            dma((WAVES, 4)),
            dma((WAVES,)),
            dma((WAVES, 5)),
            dma((WAVES,)),
            dma,
            dma,
            dma,
            dma,
            dma((2,)),
            dma((2,)),
            dma((2,)),
            dma((2,)),
            dma((4,)),
            dma((4,)),
            dma((8,)),
            dma((8,)),
            dma,
            dma,
        ],
        compiler_params=pltpu.CompilerParams(collective_id=0, has_side_effects=True),
    )(stream, norm_gain, jnp.swapaxes(in_weight, 1, 2), out_weight, docs.reshape(NZ, LANES))


def solution(mesh):
    return jax.shard_map(
        per_device,
        mesh=mesh,
        in_specs=(P("tp", "sp"), P(None, "tp"), P(None, "sp", "tp"), P(None, "tp", "sp"), P("sp")),
        out_specs=P("tp", "sp"),
        check_vma=False,
    )
```

```python
import jax
import jax.numpy as jnp
from jax import lax
from jax.experimental import pallas as pl
from jax.experimental.pallas import tpu as pltpu
from jax.sharding import PartitionSpec as P

D = 2048
PW = 1024
LAYERS = 2
NY, NX, NZ = 4, 4, 8
TOK = 128
HALO = 32
ROWS = TOK + HALO
LANES = 128
WAVES = 4
HALF = 32

MESH = pl.DeviceIdType.MESH
NT = (((1,), (1,)), ((), ()))
NN = (((1,), (0,)), ((), ()))

STEP_OFFSETS = ((0,), (-1, 1), (-2, 2), (-3, 3), (4,))


def kernel(
    stream_hbm,
    gain_hbm,
    in_w,
    out_w,
    docs_hbm,
    out,
    stream,
    gain,
    docs,
    weights,
    turned,
    taken,
    gains,
    own_gain,
    edge_docs,
    residual,
    normed,
    sums_out,
    sums_in,
    last_out,
    last_in,
    mixed,
    masks,
    counts,
    load,
    plane_send,
    plane_recv,
    z_send,
    z_recv,
    line_send,
    line_recv,
    far_recv,
    take_send,
    take_recv,
    gain_send,
    gain_recv,
    edge_send,
    edge_recv,
    pair_send,
    pair_recv,
    sums_send,
    sums_recv,
    last_send,
    last_recv,
    mixed_send,
    mixed_recv,
):
    sp = lax.axis_index("sp")
    tp = lax.axis_index("tp")
    y, x = sp // NX, sp % NX
    z, core = tp // 2, tp % 2

    def at(yy, xx, zz):
        return (yy * NX + xx, zz * 2 + core)

    def turn(value, by, size):
        return (value + by + size) % size

    sibling = (sp, z * 2 + 1 - core)
    has_next = jnp.logical_and(z == NZ - 1, sp < NY * NX - 1)
    has_edge = jnp.logical_and(z == 0, sp > 0)

    def copy(src, dst, send, recv, device):
        return pltpu.make_async_remote_copy(
            src_ref=src, dst_ref=dst, send_sem=send, recv_sem=recv, device_id=device, device_id_type=MESH
        )

    def drain(ref, sem):
        pltpu.make_async_copy(ref, ref, sem).wait()

    barrier = pltpu.get_barrier_semaphore()
    peers = [at(turn(y, d, NY), x, z) for d in range(1, NY)]
    peers += [at(y, turn(x, d, NX), z) for d in range(1, NX)]
    peers += [at(y, x, turn(z, d, NZ)) for d in range(1, NZ)]
    peers += [sibling]
    for peer in peers:
        pl.semaphore_signal(barrier, inc=1, device_id=peer, device_id_type=MESH)

    @pl.when(has_next)
    def _():
        pl.semaphore_signal(barrier, inc=1, device_id=(sp + 1, core), device_id_type=MESH)

    @pl.when(has_edge)
    def _():
        pl.semaphore_signal(
            barrier, inc=1, device_id=(sp - 1, (NZ - 1) * 2 + core), device_id_type=MESH
        )

    loads = []
    for layer in range(LAYERS):
        for i, source in enumerate((in_w, out_w)):
            w = 2 * layer + i
            loads.append(pltpu.make_async_copy(source.at[layer], weights.at[w, y, x, z], load.at[w]))
    loads.append(pltpu.make_async_copy(stream_hbm, stream, load.at[4]))
    loads.append(pltpu.make_async_copy(gain_hbm, gain, load.at[5]))
    loads.append(pltpu.make_async_copy(docs_hbm, docs, load.at[6]))
    for one in loads:
        one.start()
    for one in loads[:4]:
        one.wait()

    def turn_stream():
        for one in loads[4:]:
            one.wait()
        for j in range(NZ):
            block = stream[:, j * TOK : (j + 1) * TOK].astype(jnp.float32)
            turned[j * TOK : (j + 1) * TOK, :] = block.T.astype(jnp.bfloat16)
        own_gain[...] = jnp.zeros_like(own_gain)
        own_gain[0:LAYERS, :] = gain[...]

    extra = jnp.logical_or(has_next, has_edge).astype(jnp.int32)
    pl.semaphore_wait(barrier, len(peers) + extra)

    def send_plane(group):
        waves = (slice(0, 1), slice(1, WAVES))[group]
        for d in range(1, NY):
            part = weights.at[waves, y, x, z, 0:HALF, :]
            copy(part, part, plane_send, plane_recv.at[group], at(turn(y, d, NY), x, z)).start()
        for d in range(1, NX):
            part = weights.at[waves, y, x, z, HALF : 2 * HALF, :]
            copy(part, part, plane_send, plane_recv.at[group], at(y, turn(x, d, NX), z)).start()

    def slab_a(w, xx, zz):
        return weights.at[w, :, xx, zz, 0:HALF, :]

    def slab_b(w, yy, zz):
        return weights.at[w, yy, :, zz, HALF : 2 * HALF, :]

    def ring_a(w, step):
        up, down = at(y, x, turn(z, 1, NZ)), at(y, x, turn(z, -1, NZ))
        slab = slab_a(w, x, turn(z, -step, NZ))
        copy(slab, slab, z_send.at[w], z_recv.at[0, w, step], up).start()
        if step < 3:
            slab = slab_a(w, x, turn(z, step, NZ))
            copy(slab, slab, z_send.at[w], z_recv.at[0, w, step], down).start()

    def ring_b(w, step):
        up, down = at(y, x, turn(z, 1, NZ)), at(y, x, turn(z, -1, NZ))
        slab = slab_b(w, y, turn(z, step, NZ))
        copy(slab, slab, z_send.at[w], z_recv.at[1, w, step], down).start()
        if step < 3:
            slab = slab_b(w, y, turn(z, -step, NZ))
            copy(slab, slab, z_send.at[w], z_recv.at[1, w, step], up).start()

    def line_a(w, step):
        for offset in STEP_OFFSETS[step]:
            slab = slab_a(w, x, turn(z, offset, NZ))
            for side in (1, -1):
                to = at(y, turn(x, side, NX), z)
                copy(slab, slab, line_send.at[w], line_recv.at[w, step], to).start()

    def line_b(w, step):
        for offset in STEP_OFFSETS[step]:
            slab = slab_b(w, y, turn(z, offset, NZ))
            for side in (1, -1):
                to = at(turn(y, side, NY), x, z)
                copy(slab, slab, line_send.at[w], line_recv.at[w, step], to).start()

    def first_step(w):
        ring_a(w, 0)
        ring_b(w, 0)

    def along_lines(w, step):
        line_a(w, step)
        line_b(w, step)

    def ring_step(w, step):
        for part, ring in ((0, ring_a), (1, ring_b)):
            drain(weights.at[w, 0, 0, 0 : (4 if step < 4 else 2)], z_recv.at[part, w, step - 1])
            if step < 4:
                ring(w, step)

    def pass_on(w, step):
        drain(weights.at[w, 0, 0 : len(STEP_OFFSETS[step])], line_recv.at[w, step])
        for offset in STEP_OFFSETS[step]:
            zz = turn(z, offset, NZ)
            ahead = 1 - 2 * (zz % 2)
            a, b = slab_a(w, turn(x, -ahead, NX), zz), slab_b(w, turn(y, -ahead, NY), zz)
            copy(a, a, line_send.at[w], far_recv.at[w], at(y, turn(x, ahead, NX), z)).start()
            copy(b, b, line_send.at[w], far_recv.at[w], at(turn(y, ahead, NY), x, z)).start()

    def wait_far(w):
        drain(weights.at[w, 0], far_recv.at[w])

    def send_taken(d):
        zz = turn(z, d, NZ)
        target = at(y, x, zz)
        copy(own_gain, gains.at[core, z], gain_send, gain_recv, target).start()

        @pl.when(zz == 0)
        def _():
            copy(
                turned.at[0:TOK, :], taken.at[core, z, HALO:ROWS, :], take_send, take_recv, target
            ).start()

        @pl.when(zz > 0)
        def _():
            first = pl.multiple_of(jnp.maximum(zz * TOK - HALO, 0), 32)
            copy(
                turned.at[pl.ds(first, ROWS), :], taken.at[core, z], take_send, take_recv, target
            ).start()

    def gather_stream():
        gains[core, z] = own_gain[...]

        @pl.when(z == 0)
        def _():
            taken[core, z, HALO:ROWS, :] = turned[0:TOK, :]

        @pl.when(z > 0)
        def _():
            first = pl.multiple_of(jnp.maximum(z * TOK - HALO, 0), 32)
            taken[core, z] = turned[pl.ds(first, ROWS), :]

        drain(gains.at[0, 0:7], gain_recv)

        @pl.when(z == 0)
        def _():
            drain(taken.at[0, 0:7, HALO:ROWS, :], take_recv)

        @pl.when(z > 0)
        def _():
            drain(taken.at[0, 0:7], take_recv)

        to_next = copy(
            taken.at[core, :, TOK:ROWS, :],
            taken.at[core, :, 0:HALO, :],
            edge_send.at[0],
            edge_recv.at[0],
            (sp + 1, core),
        )
        docs_next = copy(docs, edge_docs, edge_send.at[1], edge_recv.at[1], (sp + 1, core))

        @pl.when(has_next)
        def _():
            to_next.start()
            docs_next.start()
            to_next.wait_send()
            docs_next.wait_send()

        @pl.when(has_edge)
        def _():
            to_next.wait_recv()
            docs_next.wait_recv()

        @pl.when(jnp.logical_and(z == 0, sp == 0))
        def _():
            taken[core, :, 0:HALO, :] = jnp.zeros((NZ, HALO, LANES), jnp.bfloat16)
            edge_docs[...] = jnp.full(edge_docs.shape, -1, jnp.int32)

        mine = taken.at[core]
        copy(mine, mine, pair_send.at[0], pair_recv.at[0], sibling).start()
        mine = gains.at[core]
        copy(mine, mine, pair_send.at[1], pair_recv.at[1], sibling).start()

    def windows():
        own = docs[pl.ds(z, 1), :].astype(jnp.float32)
        inside = docs[pl.ds(turn(z, -1, NZ), 1), :].astype(jnp.float32)

        def stood(row):
            return jnp.broadcast_to(row, (LANES, LANES)).T

        masks[HALO:ROWS, :] = stood(own)

        @pl.when(z > 0)
        def _():
            masks[0:HALO, :] = stood(inside)[LANES - HALO :, :]

        @pl.when(z == 0)
        def _():
            masks[0:HALO, :] = stood(edge_docs[NZ - 1 : NZ, :].astype(jnp.float32))[LANES - HALO :, :]

        column = masks[...]
        members = jnp.ones((ROWS, LANES), jnp.float32)
        for g in range(4):
            same = column == pltpu.roll(column, 2**g, 0)
            members = members + jnp.where(same, pltpu.roll(members, 2**g, 0), 0.0)
            counts[g] = members

    def same_doc(g):
        column = masks[...]
        return column == pltpu.roll(column, 2**g, 0)

    def block_of(k):
        return k % 2, k // 2

    def stream_in():
        pltpu.make_async_copy(taken.at[0], taken.at[0], pair_recv.at[0]).wait()
        pltpu.make_async_copy(gains.at[0], gains.at[0], pair_recv.at[1]).wait()
        for k in range(16):
            residual[block_of(k)] = taken[block_of(k)].astype(jnp.float32)

    def normalize(layer):
        squares = jnp.zeros((ROWS, LANES), jnp.float32)
        for k in range(16):
            r = residual[block_of(k)]
            squares = squares + r * r
        mean = jnp.sum(squares, axis=1, keepdims=True) * (1.0 / D)
        scale = lax.rsqrt(mean + 1e-06)
        for k in range(16):
            g = gains[k % 2, k // 2, layer : layer + 1, :]
            side = slice((k % 2) * LANES, (k % 2 + 1) * LANES)
            normed[k // 2, :, side] = (residual[block_of(k)] * scale * g).astype(jnp.bfloat16)

    def pooled_of(layer):
        total = jnp.zeros((ROWS, PW // 2), jnp.float32)
        for j in range(8):
            sides = [weights[2 * layer, k // NX, k % NX].reshape(PW // 2, LANES) for k in (2 * j, 2 * j + 1)]
            total = total + lax.dot_general(
                normed[j], jnp.concatenate(sides, axis=1), NT, preferred_element_type=jnp.float32
            )
        pool_in = total.astype(jnp.bfloat16).astype(jnp.float32)
        groups = []
        for g in range(4):
            values = pool_in[:, g * LANES : (g + 1) * LANES]
            window = values
            for h in range(g + 1):
                window = window + jnp.where(same_doc(h), pltpu.roll(window, 2**h, 0), 0.0)
            groups.append((window / counts[g] - values).astype(jnp.bfloat16))
        return jnp.concatenate(groups, axis=1)

    def project_out(pooled):
        for j in range(8):
            side = [weights[1, k // NX, k % NX].reshape(PW // 2, LANES) for k in (2 * j, 2 * j + 1)]
            part = lax.dot_general(
                pooled, jnp.concatenate(side, axis=1), NN, preferred_element_type=jnp.float32
            )
            for h in range(2):
                piece = part[:, h * LANES : (h + 1) * LANES]
                residual[h, j] = residual[h, j] + piece
                sums_out[j, h] = piece.astype(jnp.bfloat16)
            if j % 2 == 1:
                pair = pl.ds(j - 1, 2)
                copy(
                    sums_out.at[pair], sums_in.at[pair], sums_send.at[j // 2], sums_recv.at[j // 2], sibling
                ).start()

    def add_sums():
        for q in range(4):
            pair = pl.ds(2 * q, 2)
            pltpu.make_async_copy(sums_in.at[pair], sums_in.at[pair], sums_recv.at[q]).wait()
            for j in (2 * q, 2 * q + 1):
                for h in range(2):
                    residual[h, j] = residual[h, j] + sums_in[j, h].astype(jnp.float32)

    mine = (core + x) % 2

    def last_pair(i):
        if i < 3:
            turned_by = (i + z) % 3
            dy, dx = turned_by + turned_by // 2, 0
        else:
            turned_by = (i + z) % 5
            beyond = turned_by // 3
            dy = (1 - beyond) * (turned_by + turned_by // 2) + 2 * beyond
            dx = 2 - 2 * beyond * (4 - turned_by)
        yy = (y + dy) % NY
        return yy, (x + dx + mine) % NX, (x + dx + 1 - mine) % NX

    def last_dot(i, tail):
        yy, x_own, x_other = last_pair(i)
        side = [weights[3, yy, xx].reshape(PW // 2, LANES) for xx in (x_own, x_other)]
        part = lax.dot_general(tail, jnp.concatenate(side, axis=1), NN, preferred_element_type=jnp.float32)
        last_out[i] = part[:, LANES:].astype(jnp.bfloat16)
        copy(last_out.at[i], last_in.at[i], last_send.at[i], last_recv.at[i], sibling).start()
        j = 2 * yy + x_own // 2
        residual[core, j, HALO:ROWS, :] = residual[core, j, HALO:ROWS, :] + part[:, :LANES]

    def last_turn(i):
        yy, x_own, _ = last_pair(i)
        j = 2 * yy + x_own // 2
        pltpu.make_async_copy(last_in.at[i], last_in.at[i], last_recv.at[i]).wait()
        done = residual[core, j, HALO:ROWS, :] + last_in[i].astype(jnp.float32)
        mixed[i] = done.T.astype(jnp.bfloat16)
        lanes = pl.ds(pl.multiple_of(z * TOK, TOK), TOK)

        @pl.when(j == z)
        def _():
            out[:, lanes] = mixed[i]

        @pl.when(j != z)
        def _():
            copy(mixed.at[i], out.at[:, lanes], mixed_send, mixed_recv, at(y, x, j)).start()

    def first_arrived(group):
        drain(weights.at[0, 0, 0, 0:3] if group == 0 else weights.at[0, 0, 0:3, 0:3], plane_recv.at[group])

    def stream_ready():
        stream_in()
        normalize(0)

    held = {}

    def project_0():
        wait_far(0)
        held["pooled"] = pooled_of(0)

    def project_1():
        wait_far(1)
        project_out(held["pooled"])

    def settle():
        add_sums()
        normalize(1)

    def project_2():
        wait_far(2)
        held["pooled"] = pooled_of(1)

    def project_3():
        tail = held["pooled"][HALO:, :]
        for i in range(3):
            last_dot(i, tail)
        for i in range(3):
            last_turn(i)
        wait_far(3)
        for i in range(3, 8):
            last_dot(i, tail)
        for i in range(3, 8):
            last_turn(i)

    send_plane(0)
    send_plane(1)
    turn_stream()
    send_taken(1)
    send_taken(7)
    send_taken(2)
    send_taken(6)
    first_arrived(0)
    first_step(0)
    along_lines(0, 0)
    first_arrived(1)
    first_step(1)
    first_step(2)
    first_step(3)
    along_lines(1, 0)
    along_lines(2, 0)
    along_lines(3, 0)
    ring_step(0, 1)
    along_lines(0, 1)
    ring_step(1, 1)
    along_lines(1, 1)
    pass_on(0, 0)
    ring_step(2, 1)
    pass_on(1, 0)
    ring_step(3, 1)
    pass_on(2, 0)
    pass_on(3, 0)
    along_lines(2, 1)
    ring_step(0, 2)
    along_lines(0, 2)
    pass_on(0, 1)
    ring_step(1, 2)
    along_lines(1, 2)
    pass_on(1, 1)
    ring_step(2, 2)
    send_taken(3)
    ring_step(3, 2)
    send_taken(5)
    ring_step(0, 3)
    along_lines(0, 3)
    pass_on(0, 2)
    ring_step(1, 3)
    along_lines(1, 3)
    pass_on(1, 2)
    ring_step(2, 3)
    send_taken(4)
    along_lines(3, 1)
    pass_on(2, 1)
    ring_step(3, 3)
    along_lines(2, 2)
    ring_step(0, 4)
    along_lines(0, 4)
    pass_on(0, 3)
    ring_step(1, 4)
    along_lines(1, 4)
    pass_on(1, 3)
    ring_step(2, 4)
    along_lines(2, 3)
    along_lines(2, 4)
    pass_on(3, 1)
    ring_step(3, 4)
    along_lines(3, 2)
    along_lines(3, 3)
    along_lines(3, 4)
    pass_on(0, 4)
    pass_on(2, 2)
    gather_stream()
    windows()
    pass_on(1, 4)
    stream_ready()
    project_0()
    pass_on(2, 3)
    pass_on(2, 4)
    pass_on(3, 2)
    project_1()
    pass_on(3, 3)
    pass_on(3, 4)
    settle()
    project_2()
    project_3()

    drain(out.at[:, 0 : 7 * TOK], mixed_recv)
    drain(mixed.at[0:7], mixed_send)
    drain(weights.at[0, 0, 0:2, 0:6], plane_send)
    for w in range(WAVES):
        drain(weights.at[w, 0, :, 0:7], z_send.at[w])
        drain(weights.at[w, 0:3], line_send.at[w])
    drain(gains.at[0, 0:7], gain_send)

    @pl.when(z == 0)
    def _():
        drain(taken.at[0, 0:7], take_send)

    @pl.when(z > 0)
    def _():
        drain(taken.at[0, :, 0 : ROWS - 24, :], take_send)

    pltpu.make_async_copy(taken.at[0], taken.at[0], pair_send.at[0]).wait()
    pltpu.make_async_copy(gains.at[0], gains.at[0], pair_send.at[1]).wait()
    for q in range(4):
        pair = pl.ds(2 * q, 2)
        pltpu.make_async_copy(sums_out.at[pair], sums_out.at[pair], sums_send.at[q]).wait()
    for i in range(8):
        pltpu.make_async_copy(last_out.at[i], last_out.at[i], last_send.at[i]).wait()


def per_device(stream, norm_gain, in_weight, out_weight, docs):
    vmem = pl.BlockSpec(memory_space=pltpu.VMEM)
    dma = pltpu.SemaphoreType.DMA
    bf16, f32 = jnp.bfloat16, jnp.float32
    return pl.pallas_call(
        kernel,
        out_shape=pltpu.VMEM(stream.shape, bf16),
        in_specs=[pl.BlockSpec(memory_space=pl.ANY)] * 5,
        out_specs=vmem,
        scratch_shapes=[
            pltpu.VMEM((LANES, NZ * TOK), bf16),
            pltpu.VMEM((LAYERS, LANES), f32),
            pltpu.VMEM((NZ, LANES), jnp.int32),
            pltpu.VMEM((WAVES, NY, NX, NZ, 64, LANES), bf16),
            pltpu.VMEM((NZ * TOK, LANES), bf16),
            pltpu.VMEM((2, NZ, ROWS, LANES), bf16),
            pltpu.VMEM((2, NZ, 8, LANES), f32),
            pltpu.VMEM((8, LANES), f32),
            pltpu.VMEM((NZ, LANES), jnp.int32),
            pltpu.VMEM((2, NZ, ROWS, LANES), f32),
            pltpu.VMEM((NZ, ROWS, 2 * LANES), bf16),
            pltpu.VMEM((NZ, 2, ROWS, LANES), bf16),
            pltpu.VMEM((NZ, 2, ROWS, LANES), bf16),
            pltpu.VMEM((NZ, TOK, LANES), bf16),
            pltpu.VMEM((NZ, TOK, LANES), bf16),
            pltpu.VMEM((NZ, TOK, LANES), bf16),
            pltpu.VMEM((ROWS, LANES), f32),
            pltpu.VMEM((4, ROWS, LANES), f32),
            dma((7,)),
            dma,
            dma((2,)),
            dma((WAVES,)),
            dma((2, WAVES, 4)),
            dma((WAVES,)),
            dma((WAVES, 5)),
            dma((WAVES,)),
            dma,
            dma,
            dma,
            dma,
            dma((2,)),
            dma((2,)),
            dma((2,)),
            dma((2,)),
            dma((4,)),
            dma((4,)),
            dma((8,)),
            dma((8,)),
            dma,
            dma,
        ],
        compiler_params=pltpu.CompilerParams(collective_id=0, has_side_effects=True),
    )(stream, norm_gain, jnp.swapaxes(in_weight, 1, 2), out_weight, docs.reshape(NZ, LANES))


def solution(mesh):
    return jax.shard_map(
        per_device,
        mesh=mesh,
        in_specs=(P("tp", "sp"), P(None, "tp"), P(None, "sp", "tp"), P(None, "tp", "sp"), P("sp")),
        out_specs=P("tp", "sp"),
        check_vma=False,
    )
```

```python
import jax
import jax.numpy as jnp
from jax import lax
from jax.experimental import pallas as pl
from jax.experimental.pallas import tpu as pltpu
from jax.sharding import PartitionSpec as P

D = 2048
PW = 1024
LAYERS = 2
NY, NX, NZ = 4, 4, 8
TOK = 128
HALO = 32
ROWS = TOK + HALO
LANES = 128
WAVES = 4
HALF = 32

MESH = pl.DeviceIdType.MESH
NT = (((1,), (1,)), ((), ()))
NN = (((1,), (0,)), ((), ()))

STEP_OFFSETS = ((0,), (-1, 1), (-2, 2), (-3, 3), (4,))


def kernel(
    stream_hbm,
    gain_hbm,
    in_w,
    out_w,
    docs_hbm,
    out,
    stream,
    gain,
    docs,
    weights,
    turned,
    taken,
    gains,
    own_gain,
    edge_docs,
    residual,
    normed,
    sums_out,
    sums_in,
    last_out,
    last_in,
    mixed,
    masks,
    counts,
    load,
    plane_send,
    plane_recv,
    z_send,
    z_recv,
    line_send,
    line_recv,
    far_recv,
    take_send,
    take_recv,
    gain_send,
    gain_recv,
    edge_send,
    edge_recv,
    pair_send,
    pair_recv,
    sums_send,
    sums_recv,
    last_send,
    last_recv,
    mixed_send,
    mixed_recv,
):
    sp = lax.axis_index("sp")
    tp = lax.axis_index("tp")
    y, x = sp // NX, sp % NX
    z, core = tp // 2, tp % 2

    def at(yy, xx, zz):
        return (yy * NX + xx, zz * 2 + core)

    def turn(value, by, size):
        return (value + by + size) % size

    sibling = (sp, z * 2 + 1 - core)
    has_next = jnp.logical_and(z == NZ - 1, sp < NY * NX - 1)
    has_edge = jnp.logical_and(z == 0, sp > 0)

    def copy(src, dst, send, recv, device):
        return pltpu.make_async_remote_copy(
            src_ref=src, dst_ref=dst, send_sem=send, recv_sem=recv, device_id=device, device_id_type=MESH
        )

    def drain(ref, sem):
        pltpu.make_async_copy(ref, ref, sem).wait()

    barrier = pltpu.get_barrier_semaphore()
    peers = [at(turn(y, d, NY), x, z) for d in range(1, NY)]
    peers += [at(y, turn(x, d, NX), z) for d in range(1, NX)]
    peers += [at(y, x, turn(z, d, NZ)) for d in range(1, NZ)]
    peers += [sibling]
    for peer in peers:
        pl.semaphore_signal(barrier, inc=1, device_id=peer, device_id_type=MESH)

    @pl.when(has_next)
    def _():
        pl.semaphore_signal(barrier, inc=1, device_id=(sp + 1, core), device_id_type=MESH)

    @pl.when(has_edge)
    def _():
        pl.semaphore_signal(
            barrier, inc=1, device_id=(sp - 1, (NZ - 1) * 2 + core), device_id_type=MESH
        )

    loads = []
    for layer in range(LAYERS):
        for i, source in enumerate((in_w, out_w)):
            w = 2 * layer + i
            loads.append(pltpu.make_async_copy(source.at[layer], weights.at[w, y, x, z], load.at[w]))
    loads.append(pltpu.make_async_copy(stream_hbm, stream, load.at[4]))
    loads.append(pltpu.make_async_copy(gain_hbm, gain, load.at[5]))
    loads.append(pltpu.make_async_copy(docs_hbm, docs, load.at[6]))
    for one in loads:
        one.start()
    for one in loads[:4]:
        one.wait()

    def turn_stream():
        for one in loads[4:]:
            one.wait()
        for j in range(NZ):
            block = stream[:, j * TOK : (j + 1) * TOK].astype(jnp.float32)
            turned[j * TOK : (j + 1) * TOK, :] = block.T.astype(jnp.bfloat16)
        own_gain[...] = jnp.zeros_like(own_gain)
        own_gain[0:LAYERS, :] = gain[...]

    extra = jnp.logical_or(has_next, has_edge).astype(jnp.int32)
    pl.semaphore_wait(barrier, len(peers) + extra)

    def send_plane(group):
        waves = (slice(0, 1), slice(1, WAVES))[group]
        for d in range(1, NY):
            part = weights.at[waves, y, x, z, 0:HALF, :]
            copy(part, part, plane_send, plane_recv.at[group], at(turn(y, d, NY), x, z)).start()
        for d in range(1, NX):
            part = weights.at[waves, y, x, z, HALF : 2 * HALF, :]
            copy(part, part, plane_send, plane_recv.at[group], at(y, turn(x, d, NX), z)).start()

    def slab_a(w, xx, zz):
        return weights.at[w, :, xx, zz, 0:HALF, :]

    def slab_b(w, yy, zz):
        return weights.at[w, yy, :, zz, HALF : 2 * HALF, :]

    def ring_a(w, step):
        up, down = at(y, x, turn(z, 1, NZ)), at(y, x, turn(z, -1, NZ))
        slab = slab_a(w, x, turn(z, -step, NZ))
        copy(slab, slab, z_send.at[w], z_recv.at[0, w, step], up).start()
        if step < 3:
            slab = slab_a(w, x, turn(z, step, NZ))
            copy(slab, slab, z_send.at[w], z_recv.at[0, w, step], down).start()

    def ring_b(w, step):
        up, down = at(y, x, turn(z, 1, NZ)), at(y, x, turn(z, -1, NZ))
        slab = slab_b(w, y, turn(z, step, NZ))
        copy(slab, slab, z_send.at[w], z_recv.at[1, w, step], down).start()
        if step < 3:
            slab = slab_b(w, y, turn(z, -step, NZ))
            copy(slab, slab, z_send.at[w], z_recv.at[1, w, step], up).start()

    def line_a(w, step):
        for offset in STEP_OFFSETS[step]:
            slab = slab_a(w, x, turn(z, offset, NZ))
            for side in (1, -1):
                to = at(y, turn(x, side, NX), z)
                copy(slab, slab, line_send.at[w], line_recv.at[w, step], to).start()

    def line_b(w, step):
        for offset in STEP_OFFSETS[step]:
            slab = slab_b(w, y, turn(z, offset, NZ))
            for side in (1, -1):
                to = at(turn(y, side, NY), x, z)
                copy(slab, slab, line_send.at[w], line_recv.at[w, step], to).start()

    def first_step(w):
        ring_a(w, 0)
        ring_b(w, 0)

    def along_lines(w, step):
        line_a(w, step)
        line_b(w, step)

    def ring_step(w, step):
        for part, ring in ((0, ring_a), (1, ring_b)):
            drain(weights.at[w, 0, 0, 0 : (4 if step < 4 else 2)], z_recv.at[part, w, step - 1])
            if step < 4:
                ring(w, step)

    def pass_on(w, step):
        drain(weights.at[w, 0, 0 : len(STEP_OFFSETS[step])], line_recv.at[w, step])
        for offset in STEP_OFFSETS[step]:
            zz = turn(z, offset, NZ)
            ahead = 1 - 2 * (zz % 2)
            a, b = slab_a(w, turn(x, -ahead, NX), zz), slab_b(w, turn(y, -ahead, NY), zz)
            copy(a, a, line_send.at[w], far_recv.at[w], at(y, turn(x, ahead, NX), z)).start()
            copy(b, b, line_send.at[w], far_recv.at[w], at(turn(y, ahead, NY), x, z)).start()

    def wait_far(w):
        drain(weights.at[w, 0], far_recv.at[w])

    def send_taken(d):
        zz = turn(z, d, NZ)
        target = at(y, x, zz)
        copy(own_gain, gains.at[core, z], gain_send, gain_recv, target).start()

        @pl.when(zz == 0)
        def _():
            copy(
                turned.at[0:TOK, :], taken.at[core, z, HALO:ROWS, :], take_send, take_recv, target
            ).start()

        @pl.when(zz > 0)
        def _():
            first = pl.multiple_of(jnp.maximum(zz * TOK - HALO, 0), 32)
            copy(
                turned.at[pl.ds(first, ROWS), :], taken.at[core, z], take_send, take_recv, target
            ).start()

    def gather_stream():
        gains[core, z] = own_gain[...]

        @pl.when(z == 0)
        def _():
            taken[core, z, HALO:ROWS, :] = turned[0:TOK, :]

        @pl.when(z > 0)
        def _():
            first = pl.multiple_of(jnp.maximum(z * TOK - HALO, 0), 32)
            taken[core, z] = turned[pl.ds(first, ROWS), :]

        drain(gains.at[0, 0:7], gain_recv)

        @pl.when(z == 0)
        def _():
            drain(taken.at[0, 0:7, HALO:ROWS, :], take_recv)

        @pl.when(z > 0)
        def _():
            drain(taken.at[0, 0:7], take_recv)

        to_next = copy(
            taken.at[core, :, TOK:ROWS, :],
            taken.at[core, :, 0:HALO, :],
            edge_send.at[0],
            edge_recv.at[0],
            (sp + 1, core),
        )
        docs_next = copy(docs, edge_docs, edge_send.at[1], edge_recv.at[1], (sp + 1, core))

        @pl.when(has_next)
        def _():
            to_next.start()
            docs_next.start()
            to_next.wait_send()
            docs_next.wait_send()

        @pl.when(has_edge)
        def _():
            to_next.wait_recv()
            docs_next.wait_recv()

        @pl.when(jnp.logical_and(z == 0, sp == 0))
        def _():
            taken[core, :, 0:HALO, :] = jnp.zeros((NZ, HALO, LANES), jnp.bfloat16)
            edge_docs[...] = jnp.full(edge_docs.shape, -1, jnp.int32)

        mine = taken.at[core]
        copy(mine, mine, pair_send.at[0], pair_recv.at[0], sibling).start()
        mine = gains.at[core]
        copy(mine, mine, pair_send.at[1], pair_recv.at[1], sibling).start()

    def windows():
        own = docs[pl.ds(z, 1), :].astype(jnp.float32)
        inside = docs[pl.ds(turn(z, -1, NZ), 1), :].astype(jnp.float32)

        def stood(row):
            return jnp.broadcast_to(row, (LANES, LANES)).T

        masks[HALO:ROWS, :] = stood(own)

        @pl.when(z > 0)
        def _():
            masks[0:HALO, :] = stood(inside)[LANES - HALO :, :]

        @pl.when(z == 0)
        def _():
            masks[0:HALO, :] = stood(edge_docs[NZ - 1 : NZ, :].astype(jnp.float32))[LANES - HALO :, :]

        column = masks[...]
        members = jnp.ones((ROWS, LANES), jnp.float32)
        for g in range(4):
            same = column == pltpu.roll(column, 2**g, 0)
            members = members + jnp.where(same, pltpu.roll(members, 2**g, 0), 0.0)
            counts[g] = members

    def same_doc(g):
        column = masks[...]
        return column == pltpu.roll(column, 2**g, 0)

    def block_of(k):
        return k % 2, k // 2

    def stream_in():
        pltpu.make_async_copy(taken.at[0], taken.at[0], pair_recv.at[0]).wait()
        pltpu.make_async_copy(gains.at[0], gains.at[0], pair_recv.at[1]).wait()
        for k in range(16):
            residual[block_of(k)] = taken[block_of(k)].astype(jnp.float32)

    def normalize(layer):
        squares = jnp.zeros((ROWS, LANES), jnp.float32)
        for k in range(16):
            r = residual[block_of(k)]
            squares = squares + r * r
        mean = jnp.sum(squares, axis=1, keepdims=True) * (1.0 / D)
        scale = lax.rsqrt(mean + 1e-06)
        for k in range(16):
            g = gains[k % 2, k // 2, layer : layer + 1, :]
            side = slice((k % 2) * LANES, (k % 2 + 1) * LANES)
            normed[k // 2, :, side] = (residual[block_of(k)] * scale * g).astype(jnp.bfloat16)

    def pooled_of(layer):
        total = jnp.zeros((ROWS, PW // 2), jnp.float32)
        for j in range(8):
            sides = [weights[2 * layer, k // NX, k % NX].reshape(PW // 2, LANES) for k in (2 * j, 2 * j + 1)]
            total = total + lax.dot_general(
                normed[j], jnp.concatenate(sides, axis=1), NT, preferred_element_type=jnp.float32
            )
        pool_in = total.astype(jnp.bfloat16).astype(jnp.float32)
        groups = []
        for g in range(4):
            values = pool_in[:, g * LANES : (g + 1) * LANES]
            window = values
            for h in range(g + 1):
                window = window + jnp.where(same_doc(h), pltpu.roll(window, 2**h, 0), 0.0)
            groups.append((window / counts[g] - values).astype(jnp.bfloat16))
        return jnp.concatenate(groups, axis=1)

    def project_out(pooled):
        for j in range(8):
            side = [weights[1, k // NX, k % NX].reshape(PW // 2, LANES) for k in (2 * j, 2 * j + 1)]
            part = lax.dot_general(
                pooled, jnp.concatenate(side, axis=1), NN, preferred_element_type=jnp.float32
            )
            for h in range(2):
                piece = part[:, h * LANES : (h + 1) * LANES]
                residual[h, j] = residual[h, j] + piece
                sums_out[j, h] = piece.astype(jnp.bfloat16)
            if j % 2 == 1:
                pair = pl.ds(j - 1, 2)
                copy(
                    sums_out.at[pair], sums_in.at[pair], sums_send.at[j // 2], sums_recv.at[j // 2], sibling
                ).start()

    def add_sums():
        for q in range(4):
            pair = pl.ds(2 * q, 2)
            pltpu.make_async_copy(sums_in.at[pair], sums_in.at[pair], sums_recv.at[q]).wait()
            for j in (2 * q, 2 * q + 1):
                for h in range(2):
                    residual[h, j] = residual[h, j] + sums_in[j, h].astype(jnp.float32)

    mine = (core + x) % 2

    def last_pair(i):
        if i < 3:
            turned_by = (i + z) % 3
            dy, dx = turned_by + turned_by // 2, 0
        else:
            turned_by = (i + z) % 5
            beyond = turned_by // 3
            dy = (1 - beyond) * (turned_by + turned_by // 2) + 2 * beyond
            dx = 2 - 2 * beyond * (4 - turned_by)
        yy = (y + dy) % NY
        return yy, (x + dx + mine) % NX, (x + dx + 1 - mine) % NX

    def last_dot(i, tail):
        yy, x_own, x_other = last_pair(i)
        side = [weights[3, yy, xx].reshape(PW // 2, LANES) for xx in (x_own, x_other)]
        part = lax.dot_general(tail, jnp.concatenate(side, axis=1), NN, preferred_element_type=jnp.float32)
        last_out[i] = part[:, LANES:].astype(jnp.bfloat16)
        copy(last_out.at[i], last_in.at[i], last_send.at[i], last_recv.at[i], sibling).start()
        j = 2 * yy + x_own // 2
        residual[core, j, HALO:ROWS, :] = residual[core, j, HALO:ROWS, :] + part[:, :LANES]

    def last_turn(i):
        yy, x_own, _ = last_pair(i)
        j = 2 * yy + x_own // 2
        pltpu.make_async_copy(last_in.at[i], last_in.at[i], last_recv.at[i]).wait()
        done = residual[core, j, HALO:ROWS, :] + last_in[i].astype(jnp.float32)
        mixed[i] = done.T.astype(jnp.bfloat16)
        lanes = pl.ds(pl.multiple_of(z * TOK, TOK), TOK)

        @pl.when(j == z)
        def _():
            out[:, lanes] = mixed[i]

        @pl.when(j != z)
        def _():
            copy(mixed.at[i], out.at[:, lanes], mixed_send, mixed_recv, at(y, x, j)).start()

    def first_arrived(group):
        drain(weights.at[0, 0, 0, 0:3] if group == 0 else weights.at[0, 0, 0:3, 0:3], plane_recv.at[group])

    def stream_ready():
        stream_in()
        normalize(0)

    held = {}

    def project_0():
        wait_far(0)
        held["pooled"] = pooled_of(0)

    def project_1():
        wait_far(1)
        project_out(held["pooled"])

    def settle():
        add_sums()
        normalize(1)

    def project_2():
        wait_far(2)
        held["pooled"] = pooled_of(1)

    def project_3():
        tail = held["pooled"][HALO:, :]
        for i in range(3):
            last_dot(i, tail)
        for i in range(3):
            last_turn(i)
        wait_far(3)
        for i in range(3, 8):
            last_dot(i, tail)
        for i in range(3, 8):
            last_turn(i)

    send_plane(0)
    send_plane(1)
    turn_stream()
    send_taken(1)
    send_taken(7)
    send_taken(2)
    send_taken(6)
    first_arrived(0)
    first_step(0)
    along_lines(0, 0)
    first_arrived(1)
    first_step(1)
    first_step(2)
    first_step(3)
    along_lines(1, 0)
    along_lines(2, 0)
    along_lines(3, 0)
    ring_step(0, 1)
    along_lines(0, 1)
    ring_step(1, 1)
    along_lines(1, 1)
    ring_step(2, 1)
    along_lines(2, 1)
    ring_step(3, 1)
    along_lines(3, 1)
    ring_step(0, 2)
    along_lines(0, 2)
    ring_step(1, 2)
    along_lines(1, 2)
    ring_step(2, 2)
    along_lines(2, 2)
    pass_on(0, 0)
    ring_step(3, 2)
    along_lines(3, 2)
    pass_on(1, 0)
    ring_step(0, 3)
    along_lines(0, 3)
    pass_on(2, 0)
    ring_step(1, 3)
    along_lines(1, 3)
    send_taken(3)
    pass_on(3, 0)
    ring_step(2, 3)
    along_lines(2, 3)
    send_taken(5)
    pass_on(0, 1)
    ring_step(3, 3)
    along_lines(3, 3)
    send_taken(4)
    pass_on(1, 1)
    ring_step(0, 4)
    along_lines(0, 4)
    pass_on(2, 1)
    ring_step(1, 4)
    along_lines(1, 4)
    pass_on(3, 1)
    ring_step(2, 4)
    along_lines(2, 4)
    pass_on(0, 2)
    ring_step(3, 4)
    along_lines(3, 4)
    pass_on(1, 2)
    pass_on(0, 3)
    pass_on(0, 4)
    pass_on(1, 3)
    pass_on(1, 4)
    gather_stream()
    pass_on(2, 2)
    pass_on(2, 3)
    windows()
    pass_on(2, 4)
    stream_ready()
    pass_on(3, 2)
    project_0()
    pass_on(3, 3)
    pass_on(3, 4)
    project_1()
    settle()
    project_2()
    project_3()

    drain(out.at[:, 0 : 7 * TOK], mixed_recv)
    drain(mixed.at[0:7], mixed_send)
    drain(weights.at[0, 0, 0:2, 0:6], plane_send)
    for w in range(WAVES):
        drain(weights.at[w, 0, :, 0:7], z_send.at[w])
        drain(weights.at[w, 0:3], line_send.at[w])
    drain(gains.at[0, 0:7], gain_send)

    @pl.when(z == 0)
    def _():
        drain(taken.at[0, 0:7], take_send)

    @pl.when(z > 0)
    def _():
        drain(taken.at[0, :, 0 : ROWS - 24, :], take_send)

    pltpu.make_async_copy(taken.at[0], taken.at[0], pair_send.at[0]).wait()
    pltpu.make_async_copy(gains.at[0], gains.at[0], pair_send.at[1]).wait()
    for q in range(4):
        pair = pl.ds(2 * q, 2)
        pltpu.make_async_copy(sums_out.at[pair], sums_out.at[pair], sums_send.at[q]).wait()
    for i in range(8):
        pltpu.make_async_copy(last_out.at[i], last_out.at[i], last_send.at[i]).wait()


def per_device(stream, norm_gain, in_weight, out_weight, docs):
    vmem = pl.BlockSpec(memory_space=pltpu.VMEM)
    dma = pltpu.SemaphoreType.DMA
    bf16, f32 = jnp.bfloat16, jnp.float32
    return pl.pallas_call(
        kernel,
        out_shape=pltpu.VMEM(stream.shape, bf16),
        in_specs=[pl.BlockSpec(memory_space=pl.ANY)] * 5,
        out_specs=vmem,
        scratch_shapes=[
            pltpu.VMEM((LANES, NZ * TOK), bf16),
            pltpu.VMEM((LAYERS, LANES), f32),
            pltpu.VMEM((NZ, LANES), jnp.int32),
            pltpu.VMEM((WAVES, NY, NX, NZ, 64, LANES), bf16),
            pltpu.VMEM((NZ * TOK, LANES), bf16),
            pltpu.VMEM((2, NZ, ROWS, LANES), bf16),
            pltpu.VMEM((2, NZ, 8, LANES), f32),
            pltpu.VMEM((8, LANES), f32),
            pltpu.VMEM((NZ, LANES), jnp.int32),
            pltpu.VMEM((2, NZ, ROWS, LANES), f32),
            pltpu.VMEM((NZ, ROWS, 2 * LANES), bf16),
            pltpu.VMEM((NZ, 2, ROWS, LANES), bf16),
            pltpu.VMEM((NZ, 2, ROWS, LANES), bf16),
            pltpu.VMEM((NZ, TOK, LANES), bf16),
            pltpu.VMEM((NZ, TOK, LANES), bf16),
            pltpu.VMEM((NZ, TOK, LANES), bf16),
            pltpu.VMEM((ROWS, LANES), f32),
            pltpu.VMEM((4, ROWS, LANES), f32),
            dma((7,)),
            dma,
            dma((2,)),
            dma((WAVES,)),
            dma((2, WAVES, 4)),
            dma((WAVES,)),
            dma((WAVES, 5)),
            dma((WAVES,)),
            dma,
            dma,
            dma,
            dma,
            dma((2,)),
            dma((2,)),
            dma((2,)),
            dma((2,)),
            dma((4,)),
            dma((4,)),
            dma((8,)),
            dma((8,)),
            dma,
            dma,
        ],
        compiler_params=pltpu.CompilerParams(collective_id=0, has_side_effects=True),
    )(stream, norm_gain, jnp.swapaxes(in_weight, 1, 2), out_weight, docs.reshape(NZ, LANES))


def solution(mesh):
    return jax.shard_map(
        per_device,
        mesh=mesh,
        in_specs=(P("tp", "sp"), P(None, "tp"), P(None, "sp", "tp"), P(None, "tp", "sp"), P("sp")),
        out_specs=P("tp", "sp"),
        check_vma=False,
    )
```

```python
import jax
import jax.numpy as jnp
from jax import lax
from jax.experimental import pallas as pl
from jax.experimental.pallas import tpu as pltpu
from jax.sharding import PartitionSpec as P

D = 2048
PW = 1024
LAYERS = 2
NY, NX, NZ = 4, 4, 8
TOK = 128
HALO = 32
ROWS = TOK + HALO
LANES = 128
WAVES = 4
HALF = 32

MESH = pl.DeviceIdType.MESH
NT = (((1,), (1,)), ((), ()))
NN = (((1,), (0,)), ((), ()))

STEP_OFFSETS = ((0,), (-1, 1), (-2, 2), (-3, 3), (4,))


def kernel(
    stream_hbm,
    gain_hbm,
    in_w,
    out_w,
    docs_hbm,
    out,
    stream,
    gain,
    docs,
    weights,
    turned,
    taken,
    gains,
    own_gain,
    edge_docs,
    residual,
    normed,
    sums_out,
    sums_in,
    last_out,
    last_in,
    mixed,
    masks,
    counts,
    load,
    plane_send,
    plane_recv,
    z_send,
    z_recv,
    line_send,
    line_recv,
    far_recv,
    take_send,
    take_recv,
    gain_send,
    gain_recv,
    edge_send,
    edge_recv,
    pair_send,
    pair_recv,
    sums_send,
    sums_recv,
    last_send,
    last_recv,
    mixed_send,
    mixed_recv,
):
    sp = lax.axis_index("sp")
    tp = lax.axis_index("tp")
    y, x = sp // NX, sp % NX
    z, core = tp // 2, tp % 2

    def at(yy, xx, zz):
        return (yy * NX + xx, zz * 2 + core)

    def turn(value, by, size):
        return (value + by + size) % size

    sibling = (sp, z * 2 + 1 - core)
    has_next = jnp.logical_or(z < NZ - 1, sp < NY * NX - 1)
    has_edge = jnp.logical_or(z > 0, sp > 0)
    next_sp, next_z = sp + z // (NZ - 1), (z + 1) % NZ
    last_sp, last_z = sp - (NZ - 1 - z) // (NZ - 1), (z + NZ - 1) % NZ

    def copy(src, dst, send, recv, device):
        return pltpu.make_async_remote_copy(
            src_ref=src, dst_ref=dst, send_sem=send, recv_sem=recv, device_id=device, device_id_type=MESH
        )

    def drain(ref, sem):
        pltpu.make_async_copy(ref, ref, sem).wait()

    barrier = pltpu.get_barrier_semaphore()
    peers = [at(turn(y, d, NY), x, z) for d in range(1, NY)]
    peers += [at(y, turn(x, d, NX), z) for d in range(1, NX)]
    peers += [at(y, x, turn(z, d, NZ)) for d in range(1, NZ)]
    peers += [sibling]
    for peer in peers:
        pl.semaphore_signal(barrier, inc=1, device_id=peer, device_id_type=MESH)

    for c in (core, 1 - core):

        @pl.when(has_next)
        def _(c=c):
            pl.semaphore_signal(barrier, inc=1, device_id=(next_sp, next_z * 2 + c), device_id_type=MESH)

        @pl.when(has_edge)
        def _(c=c):
            pl.semaphore_signal(barrier, inc=1, device_id=(last_sp, last_z * 2 + c), device_id_type=MESH)

    loads = []
    for layer in range(LAYERS):
        for i, source in enumerate((in_w, out_w)):
            w = 2 * layer + i
            loads.append(pltpu.make_async_copy(source.at[layer], weights.at[w, y, x, z], load.at[w]))
    loads.append(pltpu.make_async_copy(stream_hbm, stream, load.at[4]))
    loads.append(pltpu.make_async_copy(gain_hbm, gain, load.at[5]))
    loads.append(pltpu.make_async_copy(docs_hbm, docs, load.at[6]))
    for one in loads:
        one.start()
    for one in loads[:4]:
        one.wait()

    def turn_stream():
        for one in loads[4:]:
            one.wait()
        for j in range(NZ):
            block = stream[:, j * TOK : (j + 1) * TOK].astype(jnp.float32)
            turned[j * TOK : (j + 1) * TOK, :] = block.T.astype(jnp.bfloat16)
        own_gain[...] = jnp.zeros_like(own_gain)
        own_gain[0:LAYERS, :] = gain[...]

    extra = 2 * has_next.astype(jnp.int32) + 2 * has_edge.astype(jnp.int32)
    pl.semaphore_wait(barrier, len(peers) + extra)

    def send_plane(group):
        waves = (slice(0, 1), slice(1, WAVES))[group]
        for d in range(1, NY):
            part = weights.at[waves, y, x, z, 0:HALF, :]
            copy(part, part, plane_send, plane_recv.at[group], at(turn(y, d, NY), x, z)).start()
        for d in range(1, NX):
            part = weights.at[waves, y, x, z, HALF : 2 * HALF, :]
            copy(part, part, plane_send, plane_recv.at[group], at(y, turn(x, d, NX), z)).start()

    def slab_a(w, xx, zz):
        return weights.at[w, :, xx, zz, 0:HALF, :]

    def slab_b(w, yy, zz):
        return weights.at[w, yy, :, zz, HALF : 2 * HALF, :]

    def ring_a(w, step):
        up, down = at(y, x, turn(z, 1, NZ)), at(y, x, turn(z, -1, NZ))
        slab = slab_a(w, x, turn(z, -step, NZ))
        copy(slab, slab, z_send.at[w], z_recv.at[0, w, step], up).start()
        if step < 3:
            slab = slab_a(w, x, turn(z, step, NZ))
            copy(slab, slab, z_send.at[w], z_recv.at[0, w, step], down).start()

    def ring_b(w, step):
        up, down = at(y, x, turn(z, 1, NZ)), at(y, x, turn(z, -1, NZ))
        slab = slab_b(w, y, turn(z, step, NZ))
        copy(slab, slab, z_send.at[w], z_recv.at[1, w, step], down).start()
        if step < 3:
            slab = slab_b(w, y, turn(z, -step, NZ))
            copy(slab, slab, z_send.at[w], z_recv.at[1, w, step], up).start()

    def line_a(w, step):
        for offset in STEP_OFFSETS[step]:
            slab = slab_a(w, x, turn(z, offset, NZ))
            for side in (1, -1):
                to = at(y, turn(x, side, NX), z)
                copy(slab, slab, line_send.at[w], line_recv.at[w, step], to).start()

    def line_b(w, step):
        for offset in STEP_OFFSETS[step]:
            slab = slab_b(w, y, turn(z, offset, NZ))
            for side in (1, -1):
                to = at(turn(y, side, NY), x, z)
                copy(slab, slab, line_send.at[w], line_recv.at[w, step], to).start()

    def first_step(w):
        ring_a(w, 0)
        ring_b(w, 0)

    def along_lines(w, step):
        line_a(w, step)
        line_b(w, step)

    def ring_step(w, step):
        for part, ring in ((0, ring_a), (1, ring_b)):
            drain(weights.at[w, 0, 0, 0 : (4 if step < 4 else 2)], z_recv.at[part, w, step - 1])
            if step < 4:
                ring(w, step)

    def pass_on(w, step):
        drain(weights.at[w, 0, 0 : len(STEP_OFFSETS[step])], line_recv.at[w, step])
        for offset in STEP_OFFSETS[step]:
            zz = turn(z, offset, NZ)
            ahead = 1 - 2 * (zz % 2)
            a, b = slab_a(w, turn(x, -ahead, NX), zz), slab_b(w, turn(y, -ahead, NY), zz)
            copy(a, a, line_send.at[w], far_recv.at[w], at(y, turn(x, ahead, NX), z)).start()
            copy(b, b, line_send.at[w], far_recv.at[w], at(turn(y, ahead, NY), x, z)).start()

    def wait_far(w):
        drain(weights.at[w, 0], far_recv.at[w])

    def send_taken(d):
        zz = turn(z, d, NZ)
        target = at(y, x, zz)
        copy(own_gain, gains.at[core, z], gain_send, gain_recv, target).start()

        block = turned.at[pl.ds(pl.multiple_of(zz * TOK, TOK), TOK), :]
        copy(block, taken.at[core, z, HALO:ROWS, :], take_send, take_recv, target).start()

    def gather_stream():
        gains[core, z] = own_gain[...]

        taken[core, z, HALO:ROWS, :] = turned[pl.ds(pl.multiple_of(z * TOK, TOK), TOK), :]
        drain(gains.at[0, 0:7], gain_recv)
        drain(taken.at[0, 0:7, HALO:ROWS, :], take_recv)

        @pl.when(has_next)
        def _():
            for one in edges(core):
                one.start()

        half = taken.at[core, :, HALO:ROWS, :]
        copy(half, half, pair_send.at[0], pair_recv.at[0], sibling).start()
        half = gains.at[core]
        copy(half, half, pair_send.at[1], pair_recv.at[1], sibling).start()

    def edges(c):
        last, first = taken.at[c, :, TOK:ROWS, :], taken.at[c, :, 0:HALO, :]
        return (
            copy(last, first, edge_send.at[0], edge_recv.at[0], (next_sp, next_z * 2 + core)),
            copy(last, first, edge_send.at[1], edge_recv.at[1], (next_sp, next_z * 2 + 1 - core)),
            copy(docs, edge_docs, edge_send.at[2], edge_recv.at[2], (next_sp, next_z * 2 + core)),
        )

    def windows():
        @pl.when(has_edge)
        def _():
            same, other, papers = edges(core)
            same.wait_recv()
            other.wait_recv()
            papers.wait_recv()

        @pl.when(jnp.logical_and(z == 0, sp == 0))
        def _():
            taken[:, :, 0:HALO, :] = jnp.zeros((2, NZ, HALO, LANES), jnp.bfloat16)
            edge_docs[...] = jnp.full(edge_docs.shape, -1, jnp.int32)

        own = docs[pl.ds(z, 1), :].astype(jnp.float32)
        inside = docs[pl.ds(turn(z, -1, NZ), 1), :].astype(jnp.float32)

        def stood(row):
            return jnp.broadcast_to(row, (LANES, LANES)).T

        masks[HALO:ROWS, :] = stood(own)

        @pl.when(z > 0)
        def _():
            masks[0:HALO, :] = stood(inside)[LANES - HALO :, :]

        @pl.when(z == 0)
        def _():
            masks[0:HALO, :] = stood(edge_docs[NZ - 1 : NZ, :].astype(jnp.float32))[LANES - HALO :, :]

        column = masks[...]
        members = jnp.ones((ROWS, LANES), jnp.float32)
        for g in range(4):
            same = column == pltpu.roll(column, 2**g, 0)
            members = members + jnp.where(same, pltpu.roll(members, 2**g, 0), 0.0)
            counts[g] = members

    def same_doc(g):
        column = masks[...]
        return column == pltpu.roll(column, 2**g, 0)

    def block_of(k):
        return k % 2, k // 2

    def stream_in():
        drain(taken.at[0, :, HALO:ROWS, :], pair_recv.at[0])
        pltpu.make_async_copy(gains.at[0], gains.at[0], pair_recv.at[1]).wait()
        for k in range(16):
            residual[block_of(k)] = taken[block_of(k)].astype(jnp.float32)

    def normalize(layer):
        squares = jnp.zeros((ROWS, LANES), jnp.float32)
        for k in range(16):
            r = residual[block_of(k)]
            squares = squares + r * r
        mean = jnp.sum(squares, axis=1, keepdims=True) * (1.0 / D)
        scale = lax.rsqrt(mean + 1e-06)
        for k in range(16):
            g = gains[k % 2, k // 2, layer : layer + 1, :]
            side = slice((k % 2) * LANES, (k % 2 + 1) * LANES)
            normed[k // 2, :, side] = (residual[block_of(k)] * scale * g).astype(jnp.bfloat16)

    def pooled_of(layer):
        total = jnp.zeros((ROWS, PW // 2), jnp.float32)
        for j in range(8):
            sides = [weights[2 * layer, k // NX, k % NX].reshape(PW // 2, LANES) for k in (2 * j, 2 * j + 1)]
            total = total + lax.dot_general(
                normed[j], jnp.concatenate(sides, axis=1), NT, preferred_element_type=jnp.float32
            )
        pool_in = total.astype(jnp.bfloat16).astype(jnp.float32)
        groups = []
        for g in range(4):
            values = pool_in[:, g * LANES : (g + 1) * LANES]
            window = values
            for h in range(g + 1):
                window = window + jnp.where(same_doc(h), pltpu.roll(window, 2**h, 0), 0.0)
            groups.append((window / counts[g] - values).astype(jnp.bfloat16))
        return jnp.concatenate(groups, axis=1)

    def project_out(pooled):
        for j in range(8):
            side = [weights[1, k // NX, k % NX].reshape(PW // 2, LANES) for k in (2 * j, 2 * j + 1)]
            part = lax.dot_general(
                pooled, jnp.concatenate(side, axis=1), NN, preferred_element_type=jnp.float32
            )
            for h in range(2):
                piece = part[:, h * LANES : (h + 1) * LANES]
                residual[h, j] = residual[h, j] + piece
                sums_out[j, h] = piece.astype(jnp.bfloat16)
            if j % 2 == 1:
                pair = pl.ds(j - 1, 2)
                copy(
                    sums_out.at[pair], sums_in.at[pair], sums_send.at[j // 2], sums_recv.at[j // 2], sibling
                ).start()

    def add_sums():
        for q in range(4):
            pair = pl.ds(2 * q, 2)
            pltpu.make_async_copy(sums_in.at[pair], sums_in.at[pair], sums_recv.at[q]).wait()
            for j in (2 * q, 2 * q + 1):
                for h in range(2):
                    residual[h, j] = residual[h, j] + sums_in[j, h].astype(jnp.float32)

    mine = (core + x) % 2

    def last_pair(i):
        if i < 3:
            turned_by = (i + z) % 3
            dy, dx = turned_by + turned_by // 2, 0
        else:
            turned_by = (i + z) % 5
            beyond = turned_by // 3
            dy = (1 - beyond) * (turned_by + turned_by // 2) + 2 * beyond
            dx = 2 - 2 * beyond * (4 - turned_by)
        yy = (y + dy) % NY
        return yy, (x + dx + mine) % NX, (x + dx + 1 - mine) % NX

    def last_dot(i, tail):
        yy, x_own, x_other = last_pair(i)
        side = [weights[3, yy, xx].reshape(PW // 2, LANES) for xx in (x_own, x_other)]
        part = lax.dot_general(tail, jnp.concatenate(side, axis=1), NN, preferred_element_type=jnp.float32)
        last_out[i] = part[:, LANES:].astype(jnp.bfloat16)
        copy(last_out.at[i], last_in.at[i], last_send.at[i], last_recv.at[i], sibling).start()
        j = 2 * yy + x_own // 2
        residual[core, j, HALO:ROWS, :] = residual[core, j, HALO:ROWS, :] + part[:, :LANES]

    def last_turn(i):
        yy, x_own, _ = last_pair(i)
        j = 2 * yy + x_own // 2
        pltpu.make_async_copy(last_in.at[i], last_in.at[i], last_recv.at[i]).wait()
        done = residual[core, j, HALO:ROWS, :] + last_in[i].astype(jnp.float32)
        mixed[i] = done.T.astype(jnp.bfloat16)
        lanes = pl.ds(pl.multiple_of(z * TOK, TOK), TOK)

        @pl.when(j == z)
        def _():
            out[:, lanes] = mixed[i]

        @pl.when(j != z)
        def _():
            copy(mixed.at[i], out.at[:, lanes], mixed_send, mixed_recv, at(y, x, j)).start()

    def first_arrived(group):
        drain(weights.at[0, 0, 0, 0:3] if group == 0 else weights.at[0, 0, 0:3, 0:3], plane_recv.at[group])

    def stream_ready():
        stream_in()
        normalize(0)

    held = {}

    def project_0():
        wait_far(0)
        held["pooled"] = pooled_of(0)

    def project_1():
        wait_far(1)
        project_out(held["pooled"])

    def settle():
        add_sums()
        normalize(1)

    def project_2():
        wait_far(2)
        held["pooled"] = pooled_of(1)

    def project_3():
        tail = held["pooled"][HALO:, :]
        for i in range(3):
            last_dot(i, tail)
        for i in range(3):
            last_turn(i)
        wait_far(3)
        for i in range(3, 8):
            last_dot(i, tail)
        for i in range(3, 8):
            last_turn(i)

    send_plane(0)
    send_plane(1)
    turn_stream()
    send_taken(1)
    send_taken(7)
    send_taken(2)
    send_taken(6)
    first_arrived(0)
    first_step(0)
    along_lines(0, 0)
    first_arrived(1)
    first_step(1)
    first_step(2)
    first_step(3)
    along_lines(1, 0)
    along_lines(2, 0)
    along_lines(3, 0)
    ring_step(0, 1)
    along_lines(0, 1)
    ring_step(1, 1)
    along_lines(1, 1)
    ring_step(2, 1)
    along_lines(2, 1)
    ring_step(3, 1)
    along_lines(3, 1)
    ring_step(0, 2)
    along_lines(0, 2)
    ring_step(1, 2)
    along_lines(1, 2)
    ring_step(2, 2)
    along_lines(2, 2)
    pass_on(0, 0)
    ring_step(3, 2)
    along_lines(3, 2)
    pass_on(1, 0)
    ring_step(0, 3)
    along_lines(0, 3)
    pass_on(2, 0)
    ring_step(1, 3)
    along_lines(1, 3)
    send_taken(3)
    pass_on(3, 0)
    ring_step(2, 3)
    along_lines(2, 3)
    send_taken(5)
    pass_on(0, 1)
    ring_step(3, 3)
    along_lines(3, 3)
    send_taken(4)
    pass_on(1, 1)
    ring_step(0, 4)
    along_lines(0, 4)
    pass_on(2, 1)
    ring_step(1, 4)
    along_lines(1, 4)
    pass_on(3, 1)
    ring_step(2, 4)
    along_lines(2, 4)
    pass_on(0, 2)
    ring_step(3, 4)
    along_lines(3, 4)
    pass_on(1, 2)
    pass_on(0, 3)
    pass_on(0, 4)
    gather_stream()
    pass_on(1, 3)
    pass_on(1, 4)
    pass_on(2, 2)
    windows()
    pass_on(2, 3)
    pass_on(2, 4)
    stream_ready()
    pass_on(3, 2)
    project_0()
    pass_on(3, 3)
    pass_on(3, 4)
    project_1()
    settle()
    project_2()
    project_3()

    drain(out.at[:, 0 : 7 * TOK], mixed_recv)
    drain(mixed.at[0:7], mixed_send)
    drain(weights.at[0, 0, 0:2, 0:6], plane_send)
    for w in range(WAVES):
        drain(weights.at[w, 0, :, 0:7], z_send.at[w])
        drain(weights.at[w, 0:3], line_send.at[w])
    drain(gains.at[0, 0:7], gain_send)

    drain(taken.at[0, 0:7, HALO:ROWS, :], take_send)

    @pl.when(has_next)
    def _():
        for one in edges(core):
            one.wait_send()

    drain(taken.at[0, :, HALO:ROWS, :], pair_send.at[0])
    pltpu.make_async_copy(gains.at[0], gains.at[0], pair_send.at[1]).wait()
    for q in range(4):
        pair = pl.ds(2 * q, 2)
        pltpu.make_async_copy(sums_out.at[pair], sums_out.at[pair], sums_send.at[q]).wait()
    for i in range(8):
        pltpu.make_async_copy(last_out.at[i], last_out.at[i], last_send.at[i]).wait()


def per_device(stream, norm_gain, in_weight, out_weight, docs):
    vmem = pl.BlockSpec(memory_space=pltpu.VMEM)
    dma = pltpu.SemaphoreType.DMA
    bf16, f32 = jnp.bfloat16, jnp.float32
    return pl.pallas_call(
        kernel,
        out_shape=pltpu.VMEM(stream.shape, bf16),
        in_specs=[pl.BlockSpec(memory_space=pl.ANY)] * 5,
        out_specs=vmem,
        scratch_shapes=[
            pltpu.VMEM((LANES, NZ * TOK), bf16),
            pltpu.VMEM((LAYERS, LANES), f32),
            pltpu.VMEM((NZ, LANES), jnp.int32),
            pltpu.VMEM((WAVES, NY, NX, NZ, 64, LANES), bf16),
            pltpu.VMEM((NZ * TOK, LANES), bf16),
            pltpu.VMEM((2, NZ, ROWS, LANES), bf16),
            pltpu.VMEM((2, NZ, 8, LANES), f32),
            pltpu.VMEM((8, LANES), f32),
            pltpu.VMEM((NZ, LANES), jnp.int32),
            pltpu.VMEM((2, NZ, ROWS, LANES), f32),
            pltpu.VMEM((NZ, ROWS, 2 * LANES), bf16),
            pltpu.VMEM((NZ, 2, ROWS, LANES), bf16),
            pltpu.VMEM((NZ, 2, ROWS, LANES), bf16),
            pltpu.VMEM((NZ, TOK, LANES), bf16),
            pltpu.VMEM((NZ, TOK, LANES), bf16),
            pltpu.VMEM((NZ, TOK, LANES), bf16),
            pltpu.VMEM((ROWS, LANES), f32),
            pltpu.VMEM((4, ROWS, LANES), f32),
            dma((7,)),
            dma,
            dma((2,)),
            dma((WAVES,)),
            dma((2, WAVES, 4)),
            dma((WAVES,)),
            dma((WAVES, 5)),
            dma((WAVES,)),
            dma,
            dma,
            dma,
            dma,
            dma((3,)),
            dma((3,)),
            dma((2,)),
            dma((2,)),
            dma((4,)),
            dma((4,)),
            dma((8,)),
            dma((8,)),
            dma,
            dma,
        ],
        compiler_params=pltpu.CompilerParams(collective_id=0, has_side_effects=True),
    )(stream, norm_gain, jnp.swapaxes(in_weight, 1, 2), out_weight, docs.reshape(NZ, LANES))


def solution(mesh):
    return jax.shard_map(
        per_device,
        mesh=mesh,
        in_specs=(P("tp", "sp"), P(None, "tp"), P(None, "sp", "tp"), P(None, "tp", "sp"), P("sp")),
        out_specs=P("tp", "sp"),
        check_vma=False,
    )
```
